128 devices in a mesh: st: 16 (over z, x), tp: 8 (over y, core).
Axes of the slice: x: 4, y: 4, z: 4, core: 2. Of those that a mesh axis runs over, the one named last changes fastest.
Arguments:
- tokens: bfloat16 [32768, 2048], P('st', 'tp'), may hold values from -48 to 48
- store: bfloat16 [512, 64, 2048], P('st'), may hold values from -48 to 48
- passage_holder_index: int32 [256, 2], P('st'), may hold values from 0 to 15, all different within a row; in each aligned block of 16 rows (0 to 15, 16 to 31, ...) at most 4 rows name the same one
- passage_slot: int32 [256, 2], P('st'), may hold values from 0 to 31
- query_weight: bfloat16 [2048, 1024], P(None, 'tp'), may hold values from -0.125 to 0.125
- key_matrix: bfloat16 [2048, 1024], P(None, 'tp'), may hold values from -0.125 to 0.125
- value_weight: bfloat16 [2048, 1024], P(None, 'tp'), may hold values from -0.125 to 0.125
- outer_gate: bfloat16 [2048, 1024], P(None, 'tp'), may hold values from -0.125 to 0.125
- inner_gate: bfloat16 [2048, 1024], P(None, 'tp'), may hold values from -0.125 to 0.125
- conv_input: bfloat16 [2048, 1024], P(None, 'tp'), may hold values from -0.125 to 0.125
- conv_taps: bfloat16 [3, 1024], P(None, 'tp'), may hold values from -3.5 to 3.5
- route_gate_projection: bfloat16 [2048, 2], replicated, may hold values from -0.125 to 0.125
- conv_out: bfloat16 [1024, 2048], P('tp'), may hold values from -0.1875 to 0.1875
- memory_out: bfloat16 [1024, 2048], P('tp'), may hold values from -0.1875 to 0.1875
Outputs:
- mixed: bfloat16 [32768, 2048], P(('st', 'tp'))
The draws below stay inside these ranges and needn't reach their ends.
Inputs may be any that keep to these rules, and one draw needn't show every extreme that they name: `passage_holder_index`: each row names 2 different owners; among the rows of one index of st (16 aligned rows) no owner is named more than 4 times, a bound that some index of st reaches.
All inputs are finite; a program needn't handle non-finite values.
Results may differ from the reference program's by a relative error of at most 0.014.
Values may be sent and summed in bfloat16 or wider, within the bound.
No kernel may reach another device: no remote copies, remote signals or barrier semaphores. Data moves between devices by JAX's collectives and lax.ppermute only.
A program may use at most 128 MiB of HBM per device.

```python
import math
import jax
import jax.numpy as jnp
import numpy as np
from jax import lax

D = 2048
HEADS = 8
HEAD_SIZE = 128
FILTER_CHANNELS = 1024
CONV_K = 3
SEQ_LEN = 256
BLOCK = 128
NPB = 2
PLEN = 64
P_DEV = 32
MEM_WIDTH = 1024
NBLK_DEV = 16
CAP = 4
TOKENS = 32768
BLOCKS = 256
PASSAGES = 512
N_ST = 16
N_TP = 8


def draw_tokens(key, part):
    first_key = jax.random.fold_in(jax.random.fold_in(key, 11), 0)
    values = jnp.clip(jax.random.normal(first_key, (TOKENS, D), jnp.float32), -4.0, 4.0)
    return values.astype(jnp.bfloat16)


def draw_store(key, part):
    first_key = jax.random.fold_in(jax.random.fold_in(key, 23), 0)
    values = jnp.clip(jax.random.normal(first_key, (PASSAGES, PLEN, D), jnp.float32), -4.0, 4.0)
    return values.astype(jnp.bfloat16)


def set_ends(values, key, smallest, high):
    shape = values.shape
    spot = [jax.random.randint(jax.random.fold_in(key, axis), (), 0, shape[axis]) for axis in range(len(shape))]
    values = values.at[tuple(spot)].set(smallest)
    longest = shape.index(max(shape))
    spot[longest] = (spot[longest] + 1) % shape[longest]
    return values.at[tuple(spot)].set(high)


def shard_levels(key, dims, pieces, low, largest):
    level = 1.0
    for dim, shards_of in pieces:
        draws = jax.random.uniform(jax.random.fold_in(jax.random.fold_in(key, 6), dim), (shards_of,), jnp.float32, low / len(pieces), largest / len(pieces))
        level = level * jnp.repeat(jnp.exp(draws), dims[dim] // shards_of).reshape((-1,) + (1,) * (len(dims) - 1 - dim))
    return level


def rank_bounds(count, skew):
    weights = [(1 << 20) // math.isqrt(standing ** skew) + 1 for standing in range(1, count + 1)]
    scale = 1 + sum(weights) // (1 << 30)
    return np.cumsum(np.array([max(1, weight // scale) for weight in weights]))


def skewed_ids(own_key, extent, amount, skew):
    listing = rank_bounds(amount, skew)
    pick = jax.random.randint(jax.random.fold_in(own_key, 1), extent, 0, int(listing[amount - 1]))
    standing = jnp.searchsorted(jnp.asarray(listing, jnp.int32), pick, side="right")
    return jax.random.permutation(jax.random.fold_in(own_key, 2), amount)[standing].astype(jnp.int32)


def assign_block(rng, own, number, rows, count, top, limit, lean):
    sequence = jax.random.permutation(rng, count)
    heavy_load, ordinary = shares(count, rows * top, limit, lean, True), shares(count, rows * top, limit, lean, False)
    places = jnp.arange(count)

    def named(tallies, rotation):
        used = int((tallies > 0).sum())
        fixed = max(1, used // 4)
        moved = fixed + (places - fixed + rotation * (used - fixed)) % max(1, count - fixed)
        return jnp.zeros((count,), jnp.int32).at[sequence[jnp.where(places < fixed, places, moved)]].set(jnp.asarray(tallies, jnp.int32))

    tallies = jnp.where(number % 4 == 0, named(heavy_load, number // 4), named(ordinary, number - number // 4 - 1))
    mixed = jax.random.permutation(jax.random.fold_in(own, 3), count)
    donor, sink = mixed[0:count // 2 * 2:2], mixed[1:count // 2 * 2:2]
    slack = jnp.minimum(tallies[donor] - 1, limit - tallies[sink]) // 2
    slack = jnp.where((donor == sequence[0]) | (sink == sequence[0]) | (tallies[sink] == 0), 0, jnp.maximum(slack, 0))
    moved = jax.random.randint(jax.random.fold_in(own, 4), (count // 2,), 0, 1 << 20) % (slack + 1)
    tallies = tallies.at[donor].add(-moved).at[sink].add(moved)
    members = jnp.searchsorted(jnp.cumsum(tallies), jnp.arange(rows * top), side="right").astype(jnp.int32)
    listing = members.reshape(top, rows).T
    listing = listing[jax.random.permutation(jax.random.fold_in(own, 1), rows)]
    rotation = jax.random.randint(jax.random.fold_in(own, 2), (rows, 1), 0, top)
    return jnp.take_along_axis(listing, (jnp.arange(top)[None, :] + rotation) % top, axis=1)


def shares(count, total, limit, slope, full):
    loads = [(1 << 20) // math.isqrt(grade ** slope) + 1 for grade in range(1, count + 1)]
    largest = limit if full else min(limit, max(-(-total // count), total * loads[0] // sum(loads)))
    least = 1 if total - largest >= count - 1 else 0
    counts, rest = [largest] + [least] * (count - 1), total - largest - least * (count - 1)
    while rest > 0:
        candidates = [i for i in range(1, count) if counts[i] < largest] or [i for i in range(1, count) if counts[i] < limit]
        pool, budget = sum([loads[i] for i in candidates]), rest
        for i in candidates:
            more = min(limit - counts[i], max(1, budget * loads[i] // pool), rest)
            counts[i] = counts[i] + more
            rest = rest - more
    return np.array(counts)


def bell_draw(rng, dims, deviation, bound, cuts=(), held_as=jnp.bfloat16):
    entries = jax.random.normal(rng, dims, jnp.float32) * deviation
    if len(cuts) > 0:
        entries = shard_levels(rng, dims, cuts, -0.22, 0.18) * entries
    return jnp.clip(entries, min=-bound, max=bound).astype(held_as)


def setup_inputs(seed: int = 0) -> dict:
    splits = jax.random.split(jax.random.key(seed), 15)
    tokens = draw_tokens(jax.random.fold_in(splits[14], 71), 0)
    store = draw_store(jax.random.fold_in(splits[14], 71), 0)
    passage_holder_index_keys = jax.random.split(jax.random.fold_in(splits[2], 1), BLOCKS // NBLK_DEV)
    passage_holder_index_turns = jax.random.permutation(jax.random.fold_in(splits[2], 3), BLOCKS // NBLK_DEV)
    passage_holder_index = jax.vmap(lambda own, number: assign_block(jax.random.fold_in(splits[2], 2), own, number, NBLK_DEV, N_ST, NPB, CAP, 2))(passage_holder_index_keys, passage_holder_index_turns).reshape((BLOCKS, NPB))
    passage_slot = set_ends(skewed_ids(splits[3], (BLOCKS, NPB), P_DEV, 2), jax.random.fold_in(splits[3], 3), 0, P_DEV - 1).astype(jnp.int32)
    query_weight = bell_draw(splits[4], (D, MEM_WIDTH), D ** -0.5, 0.125, ((1, 8),))
    key_matrix = bell_draw(splits[5], (D, MEM_WIDTH), D ** -0.5, 0.125, ((1, 8),))
    value_weight = bell_draw(splits[6], (D, MEM_WIDTH), D ** -0.5, 0.125, ((1, 8),))
    outer_gate = bell_draw(splits[7], (D, FILTER_CHANNELS), D ** -0.5, 0.125, ((1, 8),))
    inner_gate = bell_draw(splits[8], (D, FILTER_CHANNELS), D ** -0.5, 0.125, ((1, 8),))
    conv_input = bell_draw(splits[9], (D, FILTER_CHANNELS), D ** -0.5, 0.125, ((1, 8),))
    conv_taps = bell_draw(splits[10], (CONV_K, FILTER_CHANNELS), CONV_K ** -0.5, 3.5, ((1, 8),))
    route_gate_projection = bell_draw(splits[11], (D, 2), D ** -0.5, 0.125)
    conv_out = bell_draw(splits[12], (FILTER_CHANNELS, D), FILTER_CHANNELS ** -0.5, 0.1875, ((0, 8),))
    memory_out = bell_draw(splits[13], (MEM_WIDTH, D), MEM_WIDTH ** -0.5, 0.1875, ((0, 8),))
    return {"tokens": tokens, "store": store, "passage_holder_index": passage_holder_index, "passage_slot": passage_slot, "query_weight": query_weight, "key_matrix": key_matrix, "value_weight": value_weight, "outer_gate": outer_gate, "inner_gate": inner_gate, "conv_input": conv_input, "conv_taps": conv_taps, "route_gate_projection": route_gate_projection, "conv_out": conv_out, "memory_out": memory_out}


def reference(tokens, store, passage_holder_index, passage_slot, query_weight, key_matrix, value_weight, outer_gate, inner_gate, conv_input, conv_taps, route_gate_projection, conv_out, memory_out):
    queries = jnp.dot(tokens, query_weight, preferred_element_type=jnp.float32).astype(jnp.bfloat16)
    outer_part = jnp.dot(tokens, outer_gate, preferred_element_type=jnp.float32)
    inner_part = jnp.dot(tokens, inner_gate, preferred_element_type=jnp.float32)
    value_part = jnp.dot(tokens, conv_input, preferred_element_type=jnp.float32)
    branch_mix = jax.nn.sigmoid(jnp.dot(tokens, route_gate_projection, preferred_element_type=jnp.float32))
    mixed_input = (inner_part * value_part).reshape(TOKENS // SEQ_LEN, SEQ_LEN, FILTER_CHANNELS)
    padded_input = jnp.pad(mixed_input, ((0, 0), (CONV_K - 1, 0), (0, 0)))
    tap_values = conv_taps.astype(jnp.float32)
    filtered_signal = tap_values[0] * padded_input[:, 0:SEQ_LEN]
    for offset in range(1, CONV_K):
        filtered_signal = filtered_signal + tap_values[offset] * padded_input[:, offset:offset + SEQ_LEN]
    conv_branch = (outer_part * filtered_signal.reshape(TOKENS, FILTER_CHANNELS)).astype(jnp.bfloat16)

    passage_ids = (passage_holder_index * P_DEV + passage_slot).reshape(-1).astype(jnp.int32)
    memory_rows = store[passage_ids].reshape(-1, D)
    passage_key_rows = jnp.dot(memory_rows, key_matrix, preferred_element_type=jnp.float32).astype(jnp.bfloat16)
    retrieved_content_vectors = jnp.dot(memory_rows, value_weight, preferred_element_type=jnp.float32).astype(jnp.bfloat16)
    passage_key_rows = passage_key_rows.reshape(BLOCKS, NPB * PLEN, HEADS, HEAD_SIZE)
    retrieved_content_vectors = retrieved_content_vectors.reshape(BLOCKS, NPB * PLEN, HEADS, HEAD_SIZE)
    query_block_rows = queries.reshape(BLOCKS, BLOCK, HEADS, HEAD_SIZE)
    scores = jnp.einsum('bqhd,bkhd->bhqk', query_block_rows.astype(jnp.float32), passage_key_rows.astype(jnp.float32)) * (HEAD_SIZE ** -0.5)
    softmax_shares = jax.nn.softmax(scores, axis=-1).astype(jnp.bfloat16)
    memory_branch = jnp.einsum('bhqk,bkhd->bqhd', softmax_shares.astype(jnp.float32), retrieved_content_vectors.astype(jnp.float32))
    memory_branch = memory_branch.reshape(TOKENS, MEM_WIDTH).astype(jnp.bfloat16)

    conv_cols = FILTER_CHANNELS // N_TP
    head_cols = MEM_WIDTH // N_TP
    summed = jnp.zeros((TOKENS, D), jnp.float32)
    for tensor_parallel_team in range(N_TP):
        conv_slice = conv_branch[:, tensor_parallel_team * conv_cols:(tensor_parallel_team + 1) * conv_cols]
        memory_slice = memory_branch[:, tensor_parallel_team * head_cols:(tensor_parallel_team + 1) * head_cols]
        share_term = (branch_mix[:, 0:1] * jnp.dot(conv_slice, conv_out[tensor_parallel_team * conv_cols:(tensor_parallel_team + 1) * conv_cols], preferred_element_type=jnp.float32)
                      + branch_mix[:, 1:2] * jnp.dot(memory_slice, memory_out[tensor_parallel_team * head_cols:(tensor_parallel_team + 1) * head_cols], preferred_element_type=jnp.float32))
        summed = summed + lax.optimization_barrier(share_term.astype(jnp.bfloat16)).astype(jnp.float32)
    return summed.astype(jnp.bfloat16)
```

```python
import jax
import jax.numpy as jnp
from jax import lax
from jax.sharding import PartitionSpec as P

HEAD_SIZE = 128
CONV_K = 3
SEQ_LEN = 256
BLOCK = 128
NPB = 2
PLEN = 64
N_Y = 4


PLUS = [(2 * y + c, 2 * ((y + 1) % N_Y) + c) for y in range(N_Y) for c in range(2)]
MINUS = [(2 * y + c, 2 * ((y - 1) % N_Y) + c) for y in range(N_Y) for c in range(2)]
SWAP = [(2 * y + c, 2 * y + 1 - c) for y in range(N_Y) for c in range(2)]


def plus(a):
    return lax.ppermute(a, "tp", PLUS)


def minus(a):
    return lax.ppermute(a, "tp", MINUS)


def swap(a):
    return lax.ppermute(a, "tp", SWAP)


def pick(a, index, axis=0):
    return lax.dynamic_index_in_dim(a, index, axis, keepdims=False)


def dot(a, b):
    return jnp.dot(a, b, preferred_element_type=jnp.float32)


def local(
    tokens,
    store,
    passage_holder_index,
    passage_slot,
    query_weight,
    key_matrix,
    value_weight,
    outer_gate,
    inner_gate,
    conv_input,
    conv_taps,
    route_gate_projection,
    conv_out,
    memory_out,
):
    me = lax.axis_index("tp")
    y, c = me // 2, me % 2
    D = query_weight.shape[0]
    KS = tokens.shape[1]
    HW = query_weight.shape[1]

    rows = tokens.reshape(N_Y, 2, SEQ_LEN, KS)
    h0 = pick(rows, c, 1).reshape(N_Y * SEQ_LEN, KS)
    other = pick(rows, 1 - c, 1).reshape(N_Y * SEQ_LEN, KS)
    h1 = swap(other)
    a0, b0 = plus(h0), minus(h0)
    a1, b1 = plus(h1), minus(h1)
    c0, c1 = plus(a0), minus(b1)
    pieces = (h0, h1, a0, b0, a1, b1, c0, c1)

    def slice_of(dy, flip):
        chip = (y + dy) % N_Y
        return 2 * chip + (1 - c if flip else c)

    orders = (
        slice_of(0, False), slice_of(0, True), slice_of(-1, False), slice_of(1, False),
        slice_of(-1, True), slice_of(1, True), slice_of(2, False), slice_of(2, True),
    )

    w_mine = jnp.concatenate([query_weight, outer_gate, inner_gate, conv_input], axis=1)
    w_other = swap(w_mine)
    gate = jnp.pad(route_gate_projection, ((0, 0), (0, HW - 2)))
    w_all = jnp.concatenate([w_mine, w_other, gate], axis=1)
    w_all = w_all.reshape(2 * N_Y, KS, w_all.shape[1])
    o_mine = jnp.concatenate([conv_out, memory_out], axis=0)
    o_other = swap(o_mine)
    o_all = jnp.concatenate([o_mine, o_other], axis=0)
    taps_mine = conv_taps
    taps_other = swap(conv_taps)

    owners = passage_holder_index.reshape(-1)
    local_slots = passage_slot.reshape(-1)
    block_count = passage_holder_index.shape[0]
    owner_count = lax.axis_size("st")
    request_count = owners.shape[0]
    capacity = max(2, 2 * request_count // owner_count)
    one_hot = (owners[:, None] == jnp.arange(owner_count, dtype=jnp.int32)[None, :]).astype(
        jnp.int32
    )
    before = jnp.cumsum(one_hot, axis=0) - one_hot
    position = jnp.sum(before * one_hot, axis=1)
    target = owners * capacity + position
    matches = (
        target[:, None] == jnp.arange(owner_count * capacity, dtype=jnp.int32)[None, :]
    ).astype(jnp.int32)
    outgoing = jnp.sum(matches * local_slots[:, None], axis=0).reshape(owner_count, capacity)
    wanted = lax.all_to_all(outgoing, "st", split_axis=0, concat_axis=0, tiled=True)
    flat_rows = store.reshape(-1, D)
    kv = dot(flat_rows, jnp.concatenate([key_matrix, value_weight], axis=1)).astype(jnp.bfloat16)
    table = kv.reshape(store.shape[0], PLEN, 2 * HW)
    chosen = table[wanted.reshape(-1)].reshape(owner_count, capacity, PLEN, 2 * HW)
    served = lax.all_to_all(chosen, "st", split_axis=0, concat_axis=0, tiled=True)
    slot_table = served.reshape(owner_count * capacity, PLEN, 2 * HW)
    by_core = target.reshape(N_Y, 2, -1)
    kv_mine = slot_table[pick(by_core, c, 1).reshape(-1)]
    kv_send = slot_table[pick(by_core, 1 - c, 1).reshape(-1)]
    kv_other = swap(kv_send)
    kv_mine = kv_mine.reshape(block_count // 2, NPB * PLEN, 2 * HW)
    kv_other = kv_other.reshape(block_count // 2, NPB * PLEN, 2 * HW)

    acc = None
    for group in ((0, 1, 2, 3), (4, 5), (6, 7)):
        lhs = jnp.concatenate([pieces[i] for i in group], axis=1)
        rhs = jnp.concatenate([pick(w_all, orders[i]) for i in group], axis=0)
        term = dot(lhs, rhs)
        acc = term if acc is None else acc + term
    mix = jax.nn.sigmoid(acc[:, 8 * HW : 8 * HW + 2])

    def branches(p, kv_rows, taps):
        q = p[:, :HW].astype(jnp.bfloat16).reshape(block_count // 2, BLOCK, HW)
        outer, inner, value = p[:, HW : 2 * HW], p[:, 2 * HW : 3 * HW], p[:, 3 * HW : 4 * HW]
        mixed = (inner * value).reshape(N_Y, SEQ_LEN, HW)
        padded = jnp.pad(mixed, ((0, 0), (CONV_K - 1, 0), (0, 0)))
        t = taps.astype(jnp.float32)
        filtered = sum(t[k] * padded[:, k : k + SEQ_LEN] for k in range(CONV_K))
        conv = outer * filtered.reshape(N_Y * SEQ_LEN, HW)
        scores = jnp.einsum(
            "xud,xkd->xuk", q, kv_rows[:, :, :HW], preferred_element_type=jnp.float32
        ) * HEAD_SIZE ** (-0.5)
        shares = jax.nn.softmax(scores, axis=-1).astype(jnp.bfloat16)
        mem = jnp.einsum(
            "xuk,xkd->xud", shares, kv_rows[:, :, HW:], preferred_element_type=jnp.float32
        ).reshape(N_Y * SEQ_LEN, HW)
        return [(mix[:, 0:1] * conv).astype(jnp.bfloat16), (mix[:, 1:2] * mem).astype(jnp.bfloat16)]

    u = jnp.concatenate(
        branches(acc[:, : 4 * HW], kv_mine, taps_mine)
        + branches(acc[:, 4 * HW : 8 * HW], kv_other, taps_other),
        axis=1,
    ).reshape(N_Y, SEQ_LEN, 4 * HW)

    def part(dy):
        return dot(pick(u, (y + dy) % N_Y), o_all)

    half = SEQ_LEN // 2
    bf = jnp.bfloat16
    far = part(2).astype(bf)
    ra, rb = plus(far[:half]), minus(far[half:])
    np_, nm = part(1), part(-1)
    s1 = plus(np_[half:].astype(bf))
    s2 = minus(nm[:half].astype(bf))
    s3 = plus((np_[:half] + ra.astype(jnp.float32)).astype(bf))
    s4 = minus((nm[half:] + rb.astype(jnp.float32)).astype(bf))
    own = part(0)
    f32 = jnp.float32
    top = own[:half] + s2.astype(f32) + s3.astype(f32)
    bottom = own[half:] + s1.astype(f32) + s4.astype(f32)
    return jnp.concatenate([top, bottom], axis=0).astype(bf)


def solution(mesh):
    return jax.shard_map(
        local,
        mesh=mesh,
        in_specs=(
            P("st", "tp"),
            P("st", None, None),
            P("st", None),
            P("st", None),
            P(None, "tp"),
            P(None, "tp"),
            P(None, "tp"),
            P(None, "tp"),
            P(None, "tp"),
            P(None, "tp"),
            P(None, "tp"),
            P(),
            P("tp", None),
            P("tp", None),
        ),
        out_specs=P(("st", "tp"), None),
        check_vma=False,
    )
```

```python
import jax
import jax.numpy as jnp
from jax import lax
from jax.experimental import pallas as pl
from jax.experimental.pallas import tpu as pltpu
from jax.sharding import PartitionSpec as P

HEAD_SIZE = 128
SEQ_LEN = 256
BLOCK = 128
PLEN = 64
N_Y = 4
N_X = 4
N_Z = 4
BF = jnp.bfloat16
F32 = jnp.float32


SHIFT = {
    s: [(2 * y + c, 2 * ((y + s) % N_Y) + c) for y in range(N_Y) for c in range(2)]
    for s in (1, -1, 2)
}
SWAP = [(2 * y + c, 2 * y + 1 - c) for y in range(N_Y) for c in range(2)]


def plane_shift(s):
    pairs = []
    for z in range(N_Z):
        for x in range(N_X):
            for y in range(N_Y):
                for c in range(2):
                    z2, x2 = (z, (x + s) % N_X) if c == 0 else ((z + s) % N_Z, x)
                    pairs.append(((z * N_X + x) * 8 + 2 * y + c, (z2 * N_X + x2) * 8 + 2 * y + c))
    return pairs


def shift(a, s):
    return lax.ppermute(a, "tp", SHIFT[s])


def swap(a):
    return lax.ppermute(a, "tp", SWAP)


def plane(a, s):
    return lax.ppermute(a, ("st", "tp"), plane_shift(s))


def pick(a, index, axis=0):
    return lax.dynamic_index_in_dim(a, index, axis, keepdims=False)


def dot(a, b):
    return jnp.dot(a, b, preferred_element_type=F32)


def project_kernel(sc, *refs):
    pieces = refs[:8]
    wm, wo, gate, tm, to = refs[8:13]
    q_ref = refs[13]
    conv_refs = refs[14:18]
    logit_ref = refs[18]
    j = pl.program_id(0)
    acc_m = acc_o = None
    for k in range(8):
        row = pl.ds(pl.multiple_of(sc[k] * 256, 256), 256)
        x = pieces[k][...]
        am, ao = dot(x, wm[row, :]), dot(x, wo[row, :])
        acc_m = am if acc_m is None else acc_m + am
        acc_o = ao if acc_o is None else acc_o + ao
    H = HEAD_SIZE
    q_ref[:, :H] = acc_m[:, :H].astype(BF)
    q_ref[:, H:] = acc_o[:, :H].astype(BF)
    ids = lax.broadcasted_iota(jnp.int32, (SEQ_LEN, H), 0)

    def conv(acc, taps):
        t = taps[...].astype(F32)
        prod = acc[:, 2 * H : 3 * H] * acc[:, 3 * H :]
        back1 = jnp.where(ids >= 1, pltpu.roll(prod, 1, 0), 0.0)
        back2 = jnp.where(ids >= 2, pltpu.roll(prod, 2, 0), 0.0)
        filtered = t[0:1] * back2 + t[1:2] * back1 + t[2:3] * prod
        return (acc[:, H : 2 * H] * filtered).astype(BF)

    cm, co = conv(acc_m, tm), conv(acc_o, to)
    for i in range(4):

        @pl.when(j == i)
        def _(i=i):
            conv_refs[i][:, :H] = cm
            conv_refs[i][:, H:] = co

    @pl.when(j == 3)
    def _():
        acc = None
        for k in range(8):
            row = pl.ds(pl.multiple_of(sc[k] * 256, 256), 256)
            a = dot(pieces[k][...], gate[row, :])
            acc = a if acc is None else acc + a
        logit_ref[...] = acc


def project(sc, pieces, wm, wo, gate, tm, to):
    rows = pieces[0].shape[0]
    whole = lambda a: pl.BlockSpec(a.shape, lambda j, s: (0, 0))
    tile = pl.BlockSpec((SEQ_LEN, 256), lambda j, s: (s[8 + j], 0))
    fixed = lambda n: pl.BlockSpec((SEQ_LEN, n), lambda j, s: (0, 0))
    return pl.pallas_call(
        project_kernel,
        grid_spec=pltpu.PrefetchScalarGridSpec(
            num_scalar_prefetch=1,
            grid=(4,),
            in_specs=[tile] * 8 + [whole(a) for a in (wm, wo, gate, tm, to)],
            out_specs=[tile] + [fixed(256)] * 4 + [fixed(128)],
        ),
        out_shape=[jax.ShapeDtypeStruct((rows, 256), BF)]
        + [jax.ShapeDtypeStruct((SEQ_LEN, 256), BF)] * 4
        + [jax.ShapeDtypeStruct((SEQ_LEN, 128), F32)],
        compiler_params=pltpu.CompilerParams(vmem_limit_bytes=40 * 2**20),
        cost_estimate=pl.CostEstimate(
            flops=2 * rows * 2048 * 1024, bytes_accessed=9 * 2**20, transcendentals=0
        ),
        name="project",
    )(sc, *pieces, wm, wo, gate, tm, to)


def attend_kernel(sc, q, tab_m, tab_o, *outs):
    H = HEAD_SIZE
    for j in range(4):
        for half in range(2):
            b = sc[16 + j] * 2 + half
            t0, t1 = sc[2 * b], sc[2 * b + 1]
            rows = pl.ds(pl.multiple_of(b * BLOCK, BLOCK), BLOCK)
            for h, tab in enumerate((tab_m, tab_o)):
                kv = jnp.concatenate([tab[t0], tab[t1]], axis=0)
                qb = q[rows, h * H : (h + 1) * H]
                s = lax.dot_general(
                    qb, kv[:, :H], (((1,), (1,)), ((), ())), preferred_element_type=F32
                ) * (H**-0.5)
                e = jnp.exp(s - jnp.max(s, axis=-1, keepdims=True))
                p = (e / jnp.sum(e, axis=-1, keepdims=True)).astype(BF)
                o = dot(p, kv[:, H:])
                outs[j][half * BLOCK : (half + 1) * BLOCK, h * H : (h + 1) * H] = o.astype(BF)


def attend(sc, q, tab_m, tab_o):
    whole = lambda a: pl.BlockSpec(a.shape, lambda i, s, n=a.ndim: (0,) * n)
    return pl.pallas_call(
        attend_kernel,
        grid_spec=pltpu.PrefetchScalarGridSpec(
            num_scalar_prefetch=1,
            grid=(1,),
            in_specs=[whole(q), whole(tab_m), whole(tab_o)],
            out_specs=[pl.BlockSpec((SEQ_LEN, 256), lambda i, s: (0, 0))] * 4,
        ),
        out_shape=[jax.ShapeDtypeStruct((SEQ_LEN, 256), BF)] * 4,
        compiler_params=pltpu.CompilerParams(vmem_limit_bytes=40 * 2**20),
        cost_estimate=pl.CostEstimate(
            flops=3 * 10**9, bytes_accessed=5 * 2**20, transcendentals=2**18
        ),
        name="attend",
    )(sc, q, tab_m, tab_o)


def finish_kernel(sc, *refs):
    sides = (refs[0:5], refs[5:10])
    convs, mems, logits = refs[10:14], refs[14:18], refs[18]
    out = refs[19]
    w, sems = refs[20], refs[21]
    copies = []
    n = 0
    for side in range(2):
        own, e, r1, r2, r3 = sides[side]
        base = side * 128
        for branch in range(2):
            copies.append(
                pltpu.make_async_copy(
                    own.at[pl.ds(branch * 128, 128)],
                    w.at[0, branch, pl.ds(base, 128)],
                    sems.at[n],
                )
            )
            n += 1
        for src, back in ((e, 0), (r1, 3), (r2, 1), (r3, 2)):
            quarter = lax.rem(sc[side] + back, 4)
            branch = lax.div(quarter, 2)
            row = pl.multiple_of(base + lax.rem(quarter, 2) * 64, 64)
            for d in range(3):
                copies.append(
                    pltpu.make_async_copy(
                        src.at[pl.ds(d * 64, 64)],
                        w.at[1 + d, branch, pl.ds(row, 64)],
                        sems.at[n],
                    )
                )
                n += 1
    for c in copies:
        c.start()
    mix = jax.nn.sigmoid(logits[...])
    m0, m1 = mix[:, 0:1], mix[:, 1:2]
    for c in copies:
        c.wait()

    def step(i, carry):
        cols = pl.ds(pl.multiple_of(i * 512, 512), 512)
        a0 = a1 = None
        for d in range(4):
            x0 = dot(convs[d][...], w[d, 0, :, cols])
            x1 = dot(mems[d][...], w[d, 1, :, cols])
            a0 = x0 if a0 is None else a0 + x0
            a1 = x1 if a1 is None else a1 + x1
        out[:, cols] = (m0 * a0 + m1 * a1).astype(BF)
        return carry

    lax.fori_loop(0, 4, step, 0)


def finish(sc, mine, other, convs, mems, logits):
    width = mine[0].shape[1]
    hbm = pl.BlockSpec(memory_space=pl.ANY)
    whole = lambda a: pl.BlockSpec(a.shape, lambda i, s: (0, 0))
    vm = list(convs) + list(mems) + [logits]
    return pl.pallas_call(
        finish_kernel,
        grid_spec=pltpu.PrefetchScalarGridSpec(
            num_scalar_prefetch=1,
            grid=(1,),
            in_specs=[hbm] * 10 + [whole(a) for a in vm],
            out_specs=pl.BlockSpec((SEQ_LEN, width), lambda i, s: (0, 0)),
            scratch_shapes=[
                pltpu.VMEM((4, 2, 256, width), BF),
                pltpu.SemaphoreType.DMA((28,)),
            ],
        ),
        out_shape=jax.ShapeDtypeStruct((SEQ_LEN, width), BF),
        compiler_params=pltpu.CompilerParams(vmem_limit_bytes=40 * 2**20),
        cost_estimate=pl.CostEstimate(
            flops=2 * SEQ_LEN * 2048 * 2048, bytes_accessed=10 * 2**20, transcendentals=0
        ),
        name="finish",
    )(sc, *mine, *other, *vm)


def local(
    tokens,
    store,
    passage_holder_index,
    passage_slot,
    query_weight,
    key_matrix,
    value_weight,
    outer_gate,
    inner_gate,
    conv_input,
    conv_taps,
    route_gate_projection,
    conv_out,
    memory_out,
):
    me = lax.axis_index("tp")
    st = lax.axis_index("st")
    y, c = me // 2, me % 2
    z, x = st // N_X, st % N_X
    D = query_weight.shape[0]
    KS = tokens.shape[1]
    HW = query_weight.shape[1]
    i32 = jnp.int32

    o_mine = jnp.concatenate([conv_out, memory_out], axis=0)
    quarter = jnp.where(c == 0, x, z)
    quarter_other = jnp.where(c == 0, z, x)
    part = pick(o_mine.reshape(4, 64, D), quarter)
    ys = [shift(part, s) for s in (1, -1, 2)]
    e = jnp.concatenate(ys, axis=0)
    r1, r2, r3 = plane(e, 1), plane(e, -1), plane(e, 2)
    w_own = [o_mine, e, r1, r2, r3]
    w_other = [swap(a) for a in w_own]

    owners = passage_holder_index.reshape(-1)
    local_slots = passage_slot.reshape(-1)
    owner_count = lax.axis_size("st")
    request_count = owners.shape[0]
    capacity = max(2, 2 * request_count // owner_count)
    one_hot = (owners[:, None] == jnp.arange(owner_count, dtype=i32)[None, :]).astype(i32)
    before = jnp.cumsum(one_hot, axis=0) - one_hot
    position = jnp.sum(before * one_hot, axis=1)
    target = owners * capacity + position
    matches = (target[:, None] == jnp.arange(owner_count * capacity, dtype=i32)[None, :]).astype(i32)
    outgoing = jnp.sum(matches * local_slots[:, None], axis=0).reshape(owner_count, capacity)
    wanted = lax.all_to_all(outgoing, "st", split_axis=0, concat_axis=0, tiled=True)

    rows = tokens.reshape(N_Y, 2, SEQ_LEN, KS)
    h0 = pick(rows, c, 1).reshape(N_Y * SEQ_LEN, KS)
    other = pick(rows, 1 - c, 1).reshape(N_Y * SEQ_LEN, KS)
    a0, b0 = shift(h0, 1), shift(h0, -1)
    h1 = swap(other)
    a1, b1 = shift(h1, 1), shift(h1, -1)
    c0, c1 = shift(a0, 1), shift(b1, -1)
    pieces = (h0, h1, a0, b0, a1, b1, c0, c1)

    def slice_of(dy, flip):
        return 2 * ((y + dy) % N_Y) + (1 - c if flip else c)

    flips = ((0, False), (0, True), (-1, False), (1, False), (-1, True), (1, True), (2, False), (2, True))
    yord = [(y + d) % N_Y for d in (2, 1, -1, 0)]
    sc_project = jnp.stack([slice_of(*f) for f in flips] + yord).astype(i32)

    flat_rows = store.reshape(-1, D)
    kv = dot(flat_rows, jnp.concatenate([key_matrix, value_weight], axis=1)).astype(BF)
    table = kv.reshape(store.shape[0], PLEN, 2 * HW)
    chosen = table[wanted.reshape(-1)].reshape(owner_count, capacity, PLEN, 2 * HW)
    served = lax.all_to_all(chosen, "st", split_axis=0, concat_axis=0, tiled=True)
    tab_m = served.reshape(owner_count * capacity, PLEN, 2 * HW)
    tab_o = swap(tab_m)
    mine = pick(target.reshape(N_Y, 2, -1), c, 1).reshape(-1)
    sc_attend = jnp.concatenate([mine, jnp.stack(yord)]).astype(i32)

    w_mine = jnp.concatenate([query_weight, outer_gate, inner_gate, conv_input], axis=1)
    w_part = swap(w_mine)
    taps_part = swap(conv_taps)
    gate = jnp.pad(route_gate_projection, ((0, 0), (0, HW - 2)))

    q, *convs, logits = project(sc_project, pieces, w_mine, w_part, gate, conv_taps, taps_part)
    conv_all = [convs[3], shift(convs[1], 1), shift(convs[2], -1), shift(convs[0], 2)]
    mems = attend(sc_attend, q, tab_m, tab_o)
    mem_all = [mems[3], shift(mems[1], 1), shift(mems[2], -1), shift(mems[0], 2)]
    return finish(
        jnp.stack([quarter, quarter_other]).astype(i32), w_own, w_other, conv_all, mem_all, logits
    )


def solution(mesh):
    return jax.shard_map(
        local,
        mesh=mesh,
        in_specs=(
            P("st", "tp"),
            P("st", None, None),
            P("st", None),
            P("st", None),
            P(None, "tp"),
            P(None, "tp"),
            P(None, "tp"),
            P(None, "tp"),
            P(None, "tp"),
            P(None, "tp"),
            P(None, "tp"),
            P(),
            P("tp", None),
            P("tp", None),
        ),
        out_specs=P(("st", "tp"), None),
        check_vma=False,
    )
```

```python
import functools

import jax
import jax.numpy as jnp
from jax import lax
from jax.experimental import pallas as pl
from jax.experimental.pallas import tpu as pltpu
from jax.sharding import PartitionSpec as P

HEAD_SIZE = 128
SEQ_LEN = 256
BLOCK = 128
PLEN = 64
N_Y = 4
N_X = 4
N_Z = 4
BF = jnp.bfloat16
F32 = jnp.float32


SHIFT = {
    s: [(2 * y + c, 2 * ((y + s) % N_Y) + c) for y in range(N_Y) for c in range(2)]
    for s in (1, -1, 2)
}
SWAP = [(2 * y + c, 2 * y + 1 - c) for y in range(N_Y) for c in range(2)]


def plane_shift(s):
    pairs = []
    for z in range(N_Z):
        for x in range(N_X):
            for y in range(N_Y):
                for c in range(2):
                    z2, x2 = (z, (x + s) % N_X) if c == 0 else ((z + s) % N_Z, x)
                    pairs.append(((z * N_X + x) * 8 + 2 * y + c, (z2 * N_X + x2) * 8 + 2 * y + c))
    return pairs


def shift(a, s):
    return lax.ppermute(a, "tp", SHIFT[s])


def swap(a):
    return lax.ppermute(a, "tp", SWAP)


def plane(a, s):
    return lax.ppermute(a, ("st", "tp"), plane_shift(s))


def pick(a, index, axis=0):
    return lax.dynamic_index_in_dim(a, index, axis, keepdims=False)


def dot(a, b):
    return jnp.dot(a, b, preferred_element_type=F32)


def call(body, sc, ins, in_specs, outs, out_specs, scratch=(), grid=(1,), flops=0, bytes_=0, vmem=62):
    return pl.pallas_call(
        body,
        grid_spec=pltpu.PrefetchScalarGridSpec(
            num_scalar_prefetch=1,
            grid=grid,
            in_specs=in_specs,
            out_specs=out_specs,
            scratch_shapes=list(scratch),
        ),
        out_shape=[jax.ShapeDtypeStruct(shape, dtype) for shape, dtype in outs],
        compiler_params=pltpu.CompilerParams(vmem_limit_bytes=vmem * 2**20),
        cost_estimate=pl.CostEstimate(flops=flops, bytes_accessed=bytes_, transcendentals=0),
    )(sc, *ins)


def whole(a):
    return pl.BlockSpec(a.shape, lambda *_, n=a.ndim: (0,) * n)


def fixed(*shape):
    return pl.BlockSpec(shape, lambda *_, n=len(shape): (0,) * n)


HBM = pl.BlockSpec(memory_space=pl.ANY)


def part_kernel(sc, a, b, out):
    n = a.shape[0]
    out[:n] = a[...]
    out[n:] = b[...]


def weight_part(sc, conv_out, memory_out):
    n, d = conv_out.shape[0] // 4, conv_out.shape[1]
    spec = pl.BlockSpec((n, d), lambda i, s: (s[0], 0))
    return call(
        part_kernel, sc, (conv_out, memory_out), [spec, spec],
        [((2 * n, d), BF)], [fixed(2 * n, d)], bytes_=2**19, flops=10**8,
    )[0]


def pack_kernel(sc, a, b, c, out):
    n = a.shape[0]
    out[:n] = a[...]
    out[n : 2 * n] = b[...]
    out[2 * n :] = c[...]


def pack(sc, parts):
    n, d = parts[0].shape
    return call(
        pack_kernel, sc, parts, [whole(p) for p in parts],
        [((3 * n, d), BF)], [fixed(3 * n, d)], bytes_=2**20, flops=10**8,
    )[0]


def serve_kernel(sc, rows, kw, vw, out, table, w, sems):
    j = pl.program_id(0)
    H = kw.shape[1]

    @pl.when(j == 0)
    def _():
        w[:, :H] = kw[...]
        w[:, H:] = vw[...]

    per = rows.shape[0] // PLEN
    kv = dot(rows[...], w[...]).astype(BF)
    table[pl.ds(j * per, per)] = kv.reshape(per, PLEN, 2 * H)

    @pl.when(j == pl.num_programs(0) - 1)
    def _():
        n_own, cap = out.shape[0], out.shape[1]
        copies = [
            pltpu.make_async_copy(table.at[sc[o, k]], out.at[o, k], sems.at[o * cap + k])
            for o in range(n_own)
            for k in range(cap)
        ]
        for c in copies:
            c.start()
        for c in copies:
            c.wait()


def serve(wanted, store, kw, vw):
    n_own, cap = wanted.shape
    flat = store.reshape(-1, store.shape[-1])
    rows, d = flat.shape
    H = kw.shape[1]
    block = 256
    return call(
        serve_kernel, wanted, (flat, kw, vw),
        [pl.BlockSpec((block, d), lambda j, s: (j, 0)), whole(kw), whole(vw)],
        [((n_own, cap, PLEN, 2 * H), BF)], [HBM],
        scratch=[
            pltpu.VMEM((store.shape[0], PLEN, 2 * H), BF),
            pltpu.VMEM((d, 2 * H), BF),
            pltpu.SemaphoreType.DMA((n_own * cap,)),
        ],
        grid=(rows // block,), flops=2 * rows * d * 2 * H, bytes_=11 * 2**20,
    )[0]


def load_weights(sc, first, count, weights, w, sems):
    copies = []
    for k in range(count):
        row = pl.ds(pl.multiple_of(sc[first + k] * 256, 256), 256)
        for n, ref in enumerate(weights):
            copies.append(
                pltpu.make_async_copy(
                    ref.at[row], w.at[k, :, pl.ds(n * 128, 128)], sems.at[k * 8 + n]
                )
            )
    for c in copies:
        c.start()
    for c in copies:
        c.wait()


def gate_part(sc, first, pieces, gate):
    acc = None
    for k, p in enumerate(pieces):
        cols = pl.ds(pl.multiple_of(sc[first + k] * 256, 256), 256)
        a = lax.dot_general(
            p[...], gate[:, cols], (((1,), (1,)), ((), ())), preferred_element_type=F32
        )
        acc = a if acc is None else acc + a
    return acc


def project1_kernel(sc, *refs):
    pieces, weights = refs[:6], refs[6:14]
    gate, acc_ref, logit_ref, w, sems = refs[14:]
    j = pl.program_id(0)

    @pl.when(j == 0)
    def _():
        load_weights(sc, 0, 6, weights, w, sems)

    acc = None
    for k in range(6):
        a = dot(pieces[k][...], w[k])
        acc = a if acc is None else acc + a
    acc_ref[...] = acc

    @pl.when(j == 3)
    def _():
        logit_ref[...] = gate_part(sc, 0, pieces, gate)


def project2_kernel(sc, *refs):
    pieces, acc_in, weights = refs[:2], refs[2], refs[3:11]
    gate, tm, to, logit_in = refs[11:15]
    q_ref, conv_refs, logit_ref, w, sems = refs[15], refs[16:20], refs[20], refs[21], refs[22]
    j = pl.program_id(0)

    @pl.when(j == 0)
    def _():
        load_weights(sc, 6, 2, weights, w, sems)

    acc = acc_in[...]
    for k in range(2):
        acc = acc + dot(pieces[k][...], w[k])
    H = HEAD_SIZE
    ids = lax.broadcasted_iota(jnp.int32, (SEQ_LEN, H), 0)

    def conv(a, taps):
        t = taps[...].astype(F32)
        prod = a[:, 2 * H : 3 * H] * a[:, 3 * H :]
        back1 = jnp.where(ids >= 1, pltpu.roll(prod, 1, 0), 0.0)
        back2 = jnp.where(ids >= 2, pltpu.roll(prod, 2, 0), 0.0)
        filtered = t[0:1] * back2 + t[1:2] * back1 + t[2:3] * prod
        return (a[:, H : 2 * H] * filtered).astype(BF)

    q_ref[:, :H] = acc[:, :H].astype(BF)
    q_ref[:, H:] = acc[:, 4 * H : 5 * H].astype(BF)
    cm, co = conv(acc[:, : 4 * H], tm), conv(acc[:, 4 * H :], to)
    for i in range(4):

        @pl.when(j == i)
        def _(i=i):
            conv_refs[i][:, :H] = cm
            conv_refs[i][:, H:] = co

    @pl.when(j == 3)
    def _():
        logit_ref[...] = logit_in[...] + gate_part(sc, 6, pieces, gate)


TILE = lambda n: pl.BlockSpec((SEQ_LEN, n), lambda j, s: (s[8 + j], 0))


def project1(sc, pieces, weights, gate):
    rows = pieces[0].shape[0]
    return call(
        project1_kernel, sc, (*pieces, *weights, gate),
        [TILE(256)] * 6 + [HBM] * 8 + [whole(gate)],
        [((rows, 1024), F32), ((SEQ_LEN, 2), F32)], [TILE(1024), fixed(SEQ_LEN, 2)],
        scratch=[pltpu.VMEM((6, 256, 1024), BF), pltpu.SemaphoreType.DMA((48,))],
        grid=(4,), flops=2 * rows * 1536 * 1024, bytes_=10 * 2**20,
    )


def project2(sc, pieces, acc, weights, gate, tm, to, logits):
    rows = pieces[0].shape[0]
    return call(
        project2_kernel, sc, (*pieces, acc, *weights, gate, tm, to, logits),
        [TILE(256)] * 2 + [TILE(1024)] + [HBM] * 8 + [whole(a) for a in (gate, tm, to, logits)],
        [((rows, 256), BF)] + [((SEQ_LEN, 256), BF)] * 4 + [((SEQ_LEN, 2), F32)],
        [TILE(256)] + [fixed(SEQ_LEN, 256)] * 4 + [fixed(SEQ_LEN, 2)],
        scratch=[pltpu.VMEM((2, 256, 1024), BF), pltpu.SemaphoreType.DMA((16,))],
        grid=(4,), flops=2 * rows * 512 * 1024, bytes_=8 * 2**20,
    )


def attend_kernel(sc, q, tab_m, tab_o, o0, o1, o2, o3, s_ref, p_ref):
    H = HEAD_SIZE
    outs = (o0, o1, o2, o3)
    work = []
    for j in range(4):
        for half in range(2):
            b = sc[16 + j] * 2 + half
            rows = pl.ds(pl.multiple_of(b * BLOCK, BLOCK), BLOCK)
            for h, tab in enumerate((tab_m, tab_o)):
                work.append((j, half, h, tab, sc[2 * b], sc[2 * b + 1], rows))
    n = len(work)
    for i, (j, half, h, tab, t0, t1, rows) in enumerate(work):
        k = jnp.concatenate([tab[t0, :, :H], tab[t1, :, :H]], axis=0)
        s_ref[i * BLOCK : (i + 1) * BLOCK] = lax.dot_general(
            q[rows, h * H : (h + 1) * H], k, (((1,), (1,)), ((), ())), preferred_element_type=F32
        )
    for i in range(0, n, 4):
        part = slice(i * BLOCK, (i + 4) * BLOCK)
        s = s_ref[part] * (H**-0.5)
        e = jnp.exp(s - jnp.max(s, axis=-1, keepdims=True))
        p_ref[part] = (e / jnp.sum(e, axis=-1, keepdims=True)).astype(BF)
    for i, (j, half, h, tab, t0, t1, rows) in enumerate(work):
        v = jnp.concatenate([tab[t0, :, H:], tab[t1, :, H:]], axis=0)
        o = dot(p_ref[i * BLOCK : (i + 1) * BLOCK], v)
        outs[j][half * BLOCK : (half + 1) * BLOCK, h * H : (h + 1) * H] = o.astype(BF)


def attend(sc, q, tab_m, tab_o):
    return call(
        attend_kernel, sc, (q, tab_m, tab_o), [whole(q), whole(tab_m), whole(tab_o)],
        [((SEQ_LEN, 256), BF)] * 4, [fixed(SEQ_LEN, 256)] * 4,
        scratch=[pltpu.VMEM((16 * BLOCK, BLOCK), F32), pltpu.VMEM((16 * BLOCK, BLOCK), BF)],
        flops=10**9, bytes_=5 * 2**20,
    )


def finish_kernel(branch, sc, *refs):
    sides = (refs[0:5], refs[5:10])
    parts, logits = refs[10:14], refs[14]
    if branch == 0:
        before, (out, w, sems) = None, refs[15:]
    else:
        before, (out, w, sems) = refs[15], refs[16:]
    copies = []
    for side in range(2):
        own, e, r1, r2, r3 = sides[side]
        base = side * 128
        copies.append((own, w.at[0, pl.ds(base, 128)]))
        for src, back in ((e, 0), (r1, 3), (r2, 1), (r3, 2)):
            quarter = lax.rem(sc[side] + back, 4)
            row = pl.multiple_of(base + quarter * 32, 32)
            for d in range(3):
                copies.append(
                    (src.at[pl.ds(d * 64 + branch * 32, 32)], w.at[1 + d, pl.ds(row, 32)])
                )
    copies = [pltpu.make_async_copy(a, b, sems.at[n]) for n, (a, b) in enumerate(copies)]
    for c in copies:
        c.start()
    mix = jax.nn.sigmoid(logits[:, branch : branch + 1])
    for c in copies:
        c.wait()

    def step(i, carry):
        cols = pl.ds(pl.multiple_of(i * 512, 512), 512)
        acc = None
        for d in range(4):
            a = dot(parts[d][...], w[d, :, cols])
            acc = a if acc is None else acc + a
        if before is None:
            out[:, cols] = mix * acc
        else:
            out[:, cols] = (before[:, cols] + mix * acc).astype(BF)
        return carry

    lax.fori_loop(0, 4, step, 0)


def finish(branch, sc, mine, other, parts, logits, before=None):
    width = mine[0].shape[1]
    vm = list(parts) + [logits] + ([] if before is None else [before])
    return call(
        functools.partial(finish_kernel, branch), sc, (*mine, *other, *vm),
        [HBM] * 10 + [whole(a) for a in vm],
        [((SEQ_LEN, width), F32 if before is None else BF)], [fixed(SEQ_LEN, width)],
        scratch=[pltpu.VMEM((4, 256, width), BF), pltpu.SemaphoreType.DMA((26,))],
        flops=SEQ_LEN * 2048 * 2048, bytes_=7 * 2**20,
    )[0]


def local(
    tokens,
    store,
    passage_holder_index,
    passage_slot,
    query_weight,
    key_matrix,
    value_weight,
    outer_gate,
    inner_gate,
    conv_input,
    conv_taps,
    route_gate_projection,
    conv_out,
    memory_out,
):
    me = lax.axis_index("tp")
    st = lax.axis_index("st")
    y, c = me // 2, me % 2
    z, x = st // N_X, st % N_X
    KS = tokens.shape[1]
    HW = query_weight.shape[1]
    i32 = jnp.int32

    quarter = jnp.where(c == 0, x, z)
    quarter_other = jnp.where(c == 0, z, x)
    sc_quarter = jnp.stack([quarter, quarter_other]).astype(i32)
    part = weight_part(sc_quarter, conv_out, memory_out)
    ys = [shift(part, s) for s in (1, -1, 2)]
    e = pack(sc_quarter, ys)
    ring = [e, plane(e, 1), plane(e, -1), plane(e, 2)]
    ring_other = [swap(a) for a in ring]
    conv_out_other, memory_out_other = swap(conv_out), swap(memory_out)

    owners = passage_holder_index.reshape(-1)
    local_slots = passage_slot.reshape(-1)
    owner_count = lax.axis_size("st")
    request_count = owners.shape[0]
    capacity = max(2, 2 * request_count // owner_count)
    one_hot = (owners[:, None] == jnp.arange(owner_count, dtype=i32)[None, :]).astype(i32)
    before = jnp.cumsum(one_hot, axis=0) - one_hot
    position = jnp.sum(before * one_hot, axis=1)
    target = owners * capacity + position
    matches = (target[:, None] == jnp.arange(owner_count * capacity, dtype=i32)[None, :]).astype(i32)
    outgoing = jnp.sum(matches * local_slots[:, None], axis=0).reshape(owner_count, capacity)
    wanted = lax.all_to_all(outgoing, "st", split_axis=0, concat_axis=0)

    rows = tokens.reshape(N_Y, 2, SEQ_LEN, KS)
    h0 = pick(rows, c, 1).reshape(N_Y * SEQ_LEN, KS)
    other = pick(rows, 1 - c, 1).reshape(N_Y * SEQ_LEN, KS)
    a0, b0 = shift(h0, 1), shift(h0, -1)
    h1 = swap(other)
    a1, b1 = shift(h1, 1), shift(h1, -1)
    c0, c1 = shift(a0, 1), shift(b1, -1)
    pieces = (h0, h1, a0, b0, a1, b1, c0, c1)

    def slice_of(dy, flip):
        return 2 * ((y + dy) % N_Y) + (1 - c if flip else c)

    flips = ((0, False), (0, True), (-1, False), (1, False), (-1, True), (1, True), (2, False), (2, True))
    yord = [(y + d) % N_Y for d in (2, 1, -1, 0)]
    sc_project = jnp.stack([slice_of(*f) for f in flips] + yord).astype(i32)

    chosen = serve(wanted, store, key_matrix, value_weight)
    served = lax.all_to_all(chosen, "st", split_axis=0, concat_axis=0)
    tab_m = served.reshape(owner_count * capacity, PLEN, 2 * HW)
    tab_o = swap(tab_m)
    mine = pick(target.reshape(N_Y, 2, -1), c, 1).reshape(-1)
    sc_attend = jnp.concatenate([mine, jnp.stack(yord)]).astype(i32)

    w_mine = [query_weight, outer_gate, inner_gate, conv_input]
    weights = w_mine + [swap(w) for w in w_mine]
    taps_part = swap(conv_taps)
    gate = route_gate_projection.T

    acc, logits = project1(sc_project, pieces[:6], weights, gate)
    q, *convs, logits = project2(
        sc_project, pieces[6:], acc, weights, gate, conv_taps, taps_part, logits
    )
    conv_all = [convs[3], shift(convs[1], 1), shift(convs[2], -1), shift(convs[0], 2)]
    half = finish(0, sc_quarter, [conv_out] + ring, [conv_out_other] + ring_other, conv_all, logits)
    mems = attend(sc_attend, q, tab_m, tab_o)
    mem_all = [mems[3], shift(mems[1], 1), shift(mems[2], -1), shift(mems[0], 2)]
    return finish(
        1, sc_quarter, [memory_out] + ring, [memory_out_other] + ring_other, mem_all, logits, half
    )


def solution(mesh):
    return jax.shard_map(
        local,
        mesh=mesh,
        in_specs=(
            P("st", "tp"),
            P("st", None, None),
            P("st", None),
            P("st", None),
            P(None, "tp"),
            P(None, "tp"),
            P(None, "tp"),
            P(None, "tp"),
            P(None, "tp"),
            P(None, "tp"),
            P(None, "tp"),
            P(),
            P("tp", None),
            P("tp", None),
        ),
        out_specs=P(("st", "tp"), None),
        check_vma=False,
    )
```

```python
import jax
import jax.numpy as jnp
from jax import lax
from jax.experimental import pallas as pl
from jax.experimental.pallas import tpu as pltpu
from jax.sharding import PartitionSpec as P

HEAD_SIZE = 128
SEQ_LEN = 256
BLOCK = 128
NPB = 2
PLEN = 64
N_Y = 4
N_X = 4
N_Z = 4
BF = jnp.bfloat16
F32 = jnp.float32
SERVE_VMEM, PROJECT_VMEM, ATTEND_VMEM, FINISH_VMEM, SMALL_VMEM = 58, 62, 8, 14, 6


SHIFT = {
    s: [(2 * y + c, 2 * ((y + s) % N_Y) + c) for y in range(N_Y) for c in range(2)]
    for s in (1, -1, 2)
}
SWAP = [(2 * y + c, 2 * y + 1 - c) for y in range(N_Y) for c in range(2)]


def plane_shift(s):
    pairs = []
    for z in range(N_Z):
        for x in range(N_X):
            for y in range(N_Y):
                for c in range(2):
                    z2, x2 = (z, (x + s) % N_X) if c == 0 else ((z + s) % N_Z, x)
                    pairs.append(((z * N_X + x) * 8 + 2 * y + c, (z2 * N_X + x2) * 8 + 2 * y + c))
    return pairs


def shift(a, s):
    return lax.ppermute(a, "tp", SHIFT[s])


def swap(a):
    return lax.ppermute(a, "tp", SWAP)


def plane(a, s):
    return lax.ppermute(a, ("st", "tp"), plane_shift(s))


def pick(a, index, axis=0):
    return lax.dynamic_index_in_dim(a, index, axis, keepdims=False)


def dot(a, b):
    return jnp.dot(a, b, preferred_element_type=F32)


def call(body, sc, ins, in_specs, outs, out_specs, scratch=(), grid=(1,), flops=0, bytes_=0, vmem=62):
    return pl.pallas_call(
        body,
        grid_spec=pltpu.PrefetchScalarGridSpec(
            num_scalar_prefetch=1,
            grid=grid,
            in_specs=in_specs,
            out_specs=out_specs,
            scratch_shapes=list(scratch),
        ),
        out_shape=[jax.ShapeDtypeStruct(shape, dtype) for shape, dtype in outs],
        compiler_params=pltpu.CompilerParams(vmem_limit_bytes=vmem * 2**20),
        cost_estimate=pl.CostEstimate(flops=flops, bytes_accessed=bytes_, transcendentals=0),
    )(sc, *ins)


def whole(a):
    return pl.BlockSpec(a.shape, lambda *_, n=a.ndim: (0,) * n)


def fixed(*shape):
    return pl.BlockSpec(shape, lambda *_, n=len(shape): (0,) * n)


HBM = pl.BlockSpec(memory_space=pl.ANY)


def start(copies):
    for c in copies:
        c.start()


def wait(copies):
    for c in copies:
        c.wait()


def prep_kernel(sc, tokens, conv_out, memory_out, slab, other, part, sems):
    core, quarter = sc[2], sc[0]
    n = N_Y * SEQ_LEN
    pairs = []
    for j in range(N_Y):
        own = pl.multiple_of((2 * j + core) * SEQ_LEN, SEQ_LEN)
        away = pl.multiple_of((2 * j + 1 - core) * SEQ_LEN, SEQ_LEN)
        dst = pl.ds(j * SEQ_LEN, SEQ_LEN)
        pairs.append((tokens.at[pl.ds(own, SEQ_LEN)], slab.at[dst]))
        pairs.append((tokens.at[pl.ds(away, SEQ_LEN)], other.at[dst]))
    rows = pl.ds(pl.multiple_of(quarter * 32, 32), 32)
    for i, w in enumerate((conv_out, memory_out)):
        for cb in range(8):
            src = w.at[rows, pl.ds(cb * 256, 256)]
            dst = cb * 64 + i * 32
            pairs.append((src, slab.at[pl.ds(n + dst, 32)]))
            pairs.append((src, part.at[pl.ds(dst, 32)]))
    copies = [pltpu.make_async_copy(x, y, sems.at[k]) for k, (x, y) in enumerate(pairs)]
    start(copies)
    wait(copies)


def prep(sc, tokens, conv_out, memory_out):
    n, k = N_Y * SEQ_LEN, tokens.shape[1]
    return call(
        prep_kernel, sc, (tokens, conv_out, memory_out), [HBM] * 3,
        [((n + 512, k), BF), ((n, k), BF), ((512, k), BF)],
        [fixed(n + 512, k), fixed(n, k), fixed(512, k)],
        scratch=[pltpu.SemaphoreType.DMA((40,))], bytes_=3 * 2**20, flops=10**8, vmem=6,
    )


def pack_kernel(sc, a, b, c, out):
    for d, (ref, first) in enumerate(((a, ref_rows(a)), (b, ref_rows(b)), (c, 0))):
        for cb in range(8):
            out[d * 64 : (d + 1) * 64, cb * 256 : (cb + 1) * 256] = ref[
                first + cb * 64 : first + (cb + 1) * 64
            ]


def ref_rows(ref):
    return ref.shape[0] - 512


def pack(sc, parts):
    tail = lambda a: pl.BlockSpec((512, a.shape[1]), lambda i, s, n=a.shape[0] // 512: (n - 1, 0))
    return call(
        pack_kernel, sc, parts, [tail(p) for p in parts],
        [((192, 2048), BF)], [fixed(192, 2048)], bytes_=2**20, flops=10**8, vmem=SMALL_VMEM,
    )[0]


def serve_kernel(sc, rows, kw, vw, out, table, w, sems):
    j = pl.program_id(0)
    H = kw.shape[1]

    @pl.when(j == 0)
    def _():
        w[:, :H] = kw[...]
        w[:, H:] = vw[...]

    per = rows.shape[0] // PLEN
    kv = dot(rows[...], w[...]).astype(BF)
    table[pl.ds(j * per, per)] = kv.reshape(per, PLEN, 2 * H)

    @pl.when(j == pl.num_programs(0) - 1)
    def _():
        n_own, cap = out.shape[0], out.shape[1]
        copies = [
            pltpu.make_async_copy(table.at[sc[o, k]], out.at[o, k], sems.at[o * cap + k])
            for o in range(n_own)
            for k in range(cap)
        ]
        for c in copies:
            c.start()
        for c in copies:
            c.wait()


def serve(wanted, store, kw, vw):
    n_own, cap = wanted.shape
    flat = store.reshape(-1, store.shape[-1])
    rows, d = flat.shape
    H = kw.shape[1]
    block = 512
    return call(
        serve_kernel, wanted, (flat, kw, vw),
        [pl.BlockSpec((block, d), lambda j, s: (j, 0)), whole(kw), whole(vw)],
        [((n_own, cap, PLEN, 2 * H), BF)], [HBM],
        scratch=[
            pltpu.VMEM((store.shape[0], PLEN, 2 * H), BF),
            pltpu.VMEM((d, 2 * H), BF),
            pltpu.SemaphoreType.DMA((n_own * cap,)),
        ],
        grid=(rows // block,), flops=2 * rows * d * 2 * H, bytes_=11 * 2**20, vmem=SERVE_VMEM,
    )[0]


def project_kernel(sc, *refs):
    pieces, weights = refs[:8], refs[8:16]
    gate, tm, to = refs[16:19]
    q_out, conv_outs, logit_ref = refs[19], refs[20:24], refs[24]
    lhs, w, acc, q_s, conv_s, lsem, wsem, osem = refs[25:]
    H = HEAD_SIZE
    n_rows = lhs.shape[0]
    lcopy = [
        pltpu.make_async_copy(
            p.at[pl.ds(0, n_rows)],
            lhs.at[:, pl.ds(pl.multiple_of(sc[k] * 256, 256), 256)],
            lsem.at[k],
        )
        for k, p in enumerate(pieces)
    ]
    wcopy = [
        pltpu.make_async_copy(p, w.at[n // 2, :, pl.ds(n % 2 * H, H)], wsem.at[n])
        for n, p in enumerate(weights)
    ]
    start(lcopy)
    start(wcopy)
    wait(lcopy)
    wait(wcopy)

    def product(n, carry):
        acc[n] = dot(lhs[...], w[n])
        return carry

    lax.fori_loop(0, 4, product, 0)
    ids = lax.broadcasted_iota(jnp.int32, (SEQ_LEN, H), 0)
    taps = [t[...].astype(F32) for t in (tm, to)]

    def convolve(j, carry):
        rows = pl.ds(pl.multiple_of(sc[8 + j] * SEQ_LEN, SEQ_LEN), SEQ_LEN)
        for side, t in enumerate(taps):
            prod = acc[2 * side + 1, rows, :H] * acc[2 * side + 1, rows, H:]
            back1 = jnp.where(ids >= 1, pltpu.roll(prod, 1, 0), 0.0)
            back2 = jnp.where(ids >= 2, pltpu.roll(prod, 2, 0), 0.0)
            filtered = t[0:1] * back2 + t[1:2] * back1 + t[2:3] * prod
            outer = acc[2 * side, rows, H:]
            conv_s[j, :, side * H : (side + 1) * H] = (outer * filtered).astype(BF)
        return carry

    lax.fori_loop(0, 4, convolve, 0)
    ocopy = [pltpu.make_async_copy(conv_s.at[j], conv_outs[j], osem.at[j]) for j in range(4)]
    start(ocopy)
    q_s[:, :H] = acc[0, :, :H].astype(BF)
    q_s[:, H:] = acc[2, :, :H].astype(BF)
    qcopy = [pltpu.make_async_copy(q_s, q_out, osem.at[4])]
    start(qcopy)
    own = pl.ds(pl.multiple_of(sc[11] * SEQ_LEN, SEQ_LEN), SEQ_LEN)
    logit_ref[...] = lax.dot_general(
        lhs[own, :], gate[...], (((1,), (1,)), ((), ())), preferred_element_type=F32
    )
    wait(ocopy)
    wait(qcopy)


def project(sc, pieces, weights, gate, tm, to):
    rows = N_Y * SEQ_LEN
    d = gate.shape[1]
    return call(
        project_kernel, sc, (*pieces, *weights, gate, tm, to),
        [HBM] * 16 + [whole(a) for a in (gate, tm, to)],
        [((rows, 256), BF)] + [((SEQ_LEN, 256), BF)] * 4 + [((SEQ_LEN, 2), F32)],
        [HBM] * 5 + [fixed(SEQ_LEN, 2)],
        scratch=[
            pltpu.VMEM((rows, d), BF),
            pltpu.VMEM((4, d, 256), BF),
            pltpu.VMEM((4, rows, 256), F32),
            pltpu.VMEM((rows, 256), BF),
            pltpu.VMEM((4, SEQ_LEN, 256), BF),
            pltpu.SemaphoreType.DMA((8,)),
            pltpu.SemaphoreType.DMA((8,)),
            pltpu.SemaphoreType.DMA((5,)),
        ],
        flops=2 * rows * d * 1024, bytes_=10 * 2**20, vmem=PROJECT_VMEM,
    )


def attend_kernel(sc, q_in, tab_m, tab_o, *refs):
    outs = refs[:4]
    q, kv, s_ref, p_ref, sems, qsem = refs[4:]
    H = HEAD_SIZE
    qcopy = pltpu.make_async_copy(q_in, q, qsem)
    qcopy.start()
    work, copies = [], []
    for j in range(4):
        for half in range(2):
            b = sc[16 + j] * 2 + half
            rows = pl.ds(pl.multiple_of(b * BLOCK, BLOCK), BLOCK)
            for h, tab in enumerate((tab_m, tab_o)):
                i = len(work)
                for n in range(NPB):
                    copies.append(
                        pltpu.make_async_copy(
                            tab.at[sc[NPB * b + n]],
                            kv.at[i, pl.ds(n * PLEN, PLEN)],
                            sems.at[NPB * i + n],
                        )
                    )
                work.append((j, half, h, rows))
    start(copies)
    qcopy.wait()
    wait(copies)
    n = len(work)
    for i, (j, half, h, rows) in enumerate(work):
        s_ref[i * BLOCK : (i + 1) * BLOCK] = lax.dot_general(
            q[rows, h * H : (h + 1) * H], kv[i, :, :H], (((1,), (1,)), ((), ())),
            preferred_element_type=F32,
        )
    for i in range(0, n, 4):
        part = slice(i * BLOCK, (i + 4) * BLOCK)
        s = s_ref[part] * (H**-0.5)
        e = jnp.exp(s - jnp.max(s, axis=-1, keepdims=True))
        p_ref[part] = (e / jnp.sum(e, axis=-1, keepdims=True)).astype(BF)
    for i, (j, half, h, rows) in enumerate(work):
        o = dot(p_ref[i * BLOCK : (i + 1) * BLOCK], kv[i, :, H:])
        outs[j][half * BLOCK : (half + 1) * BLOCK, h * H : (h + 1) * H] = o.astype(BF)


def attend(sc, q, tab_m, tab_o):
    n = 16
    return call(
        attend_kernel, sc, (q, tab_m, tab_o), [HBM] * 3,
        [((SEQ_LEN, 256), BF)] * 4, [fixed(SEQ_LEN, 256)] * 4,
        scratch=[
            pltpu.VMEM(q.shape, BF),
            pltpu.VMEM((n, NPB * PLEN, 256), BF),
            pltpu.VMEM((n * BLOCK, BLOCK), F32),
            pltpu.VMEM((n * BLOCK, BLOCK), BF),
            pltpu.SemaphoreType.DMA((n * NPB,)),
            pltpu.SemaphoreType.DMA,
        ],
        flops=10**9, bytes_=5 * 2**20, vmem=ATTEND_VMEM,
    )


def finish_kernel(branch, sc, *refs):
    sides = (refs[0:5], refs[5:10])
    parts, logits = refs[10:14], refs[14]
    before = None if branch == 0 else refs[15]
    out, w, x, o_s, sems, bsem, osem = refs[-7:]
    copies = []
    for side in range(2):
        own, e, r1, r2, r3 = sides[side]
        base = side * 128
        copies.append((own, w.at[pl.ds(base, 128)]))
        for src, back in ((e, 0), (r1, 3), (r2, 1), (r3, 2)):
            quarter = lax.rem(sc[side] + back, 4)
            row = pl.multiple_of(base + quarter * 32, 32)
            for d in range(3):
                copies.append(
                    (src.at[pl.ds(d * 64 + branch * 32, 32)], w.at[pl.ds((1 + d) * 256 + row, 32)])
                )
    for d in range(4):
        copies.append((parts[d], x.at[:, pl.ds(d * 256, 256)]))
    copies = [pltpu.make_async_copy(a, b, sems.at[n]) for n, (a, b) in enumerate(copies)]
    start(copies)
    if before is not None:
        bcopy = pltpu.make_async_copy(before, o_s, bsem)
        bcopy.start()
    mix = jax.nn.sigmoid(logits[:, branch : branch + 1])
    wait(copies)
    if before is not None:
        bcopy.wait()
    step = 512

    def product(i, carry):
        cols = pl.ds(pl.multiple_of(i * step, step), step)
        a = mix * dot(x[...], w[:, cols])
        if before is None:
            o_s[:, cols] = a
        else:
            refs[-8][:, cols] = (o_s[:, cols] + a).astype(BF)
        return carry

    lax.fori_loop(0, w.shape[1] // step, product, 0)
    ocopy = pltpu.make_async_copy(o_s if before is None else refs[-8], out, osem.at[0])
    ocopy.start()
    ocopy.wait()


def finish(branch, sc, mine, other, parts, logits, before=None):
    width = mine[0].shape[1]
    last = before is not None
    ins = (*mine, *other, *parts, logits) + ((before,) if last else ())
    scratch = [
        pltpu.VMEM((1024, width), BF),
        pltpu.VMEM((SEQ_LEN, 1024), BF),
        pltpu.VMEM((SEQ_LEN, width), F32),
        pltpu.SemaphoreType.DMA((30,)),
        pltpu.SemaphoreType.DMA,
        pltpu.SemaphoreType.DMA((width // 512,)),
    ]

    def body(*refs):
        if not last:
            return finish_kernel(branch, *refs)
        return finish_kernel(branch, *refs[:-8], refs[-1], *refs[-8:-1])

    return call(
        body, sc, ins,
        [HBM] * 14 + [whole(logits)] + ([HBM] if last else []),
        [((SEQ_LEN, width), BF if last else F32)], [HBM],
        scratch=scratch + ([pltpu.VMEM((SEQ_LEN, width), BF)] if last else []),
        flops=SEQ_LEN * 2048 * 2048, bytes_=7 * 2**20, vmem=FINISH_VMEM,
    )[0]


def local(
    tokens,
    store,
    passage_holder_index,
    passage_slot,
    query_weight,
    key_matrix,
    value_weight,
    outer_gate,
    inner_gate,
    conv_input,
    conv_taps,
    route_gate_projection,
    conv_out,
    memory_out,
):
    me = lax.axis_index("tp")
    st = lax.axis_index("st")
    y, c = me // 2, me % 2
    z, x = st // N_X, st % N_X
    HW = query_weight.shape[1]
    i32 = jnp.int32

    quarter = jnp.where(c == 0, x, z)
    quarter_other = jnp.where(c == 0, z, x)
    sc_quarter = jnp.stack([quarter, quarter_other, c]).astype(i32)
    slab, other, part = prep(sc_quarter, tokens, conv_out, memory_out)

    a0, b0 = shift(slab, 1), shift(slab, -1)
    h1 = swap(other)
    far_part = shift(part, 2)
    a1, b1 = shift(h1, 1), shift(h1, -1)
    c0, c1 = shift(a0, 1), shift(b1, -1)
    pieces = (slab, h1, a0, b0, a1, b1, c0, c1)

    e = pack(sc_quarter, (a0, b0, far_part))
    ring = [e, plane(e, 1), plane(e, -1), plane(e, 2)]
    ring_other = [swap(a) for a in ring]
    conv_out_other, memory_out_other = swap(conv_out), swap(memory_out)

    owners = passage_holder_index.reshape(-1)
    local_slots = passage_slot.reshape(-1)
    owner_count = lax.axis_size("st")
    request_count = owners.shape[0]
    capacity = max(2, 2 * request_count // owner_count)
    one_hot = (owners[:, None] == jnp.arange(owner_count, dtype=i32)[None, :]).astype(i32)
    before = jnp.cumsum(one_hot, axis=0) - one_hot
    position = jnp.sum(before * one_hot, axis=1)
    target = owners * capacity + position
    matches = (target[:, None] == jnp.arange(owner_count * capacity, dtype=i32)[None, :]).astype(i32)
    outgoing = jnp.sum(matches * local_slots[:, None], axis=0).reshape(owner_count, capacity)
    wanted = lax.all_to_all(outgoing, "st", split_axis=0, concat_axis=0)

    def slice_of(dy, flip):
        return 2 * ((y + dy) % N_Y) + (1 - c if flip else c)

    flips = ((0, False), (0, True), (-1, False), (1, False), (-1, True), (1, True), (2, False), (2, True))
    yord = [(y + d) % N_Y for d in (2, 1, -1, 0)]
    sc_project = jnp.stack([slice_of(*f) for f in flips] + yord).astype(i32)

    chosen = serve(wanted, store, key_matrix, value_weight)
    served = lax.all_to_all(chosen, "st", split_axis=0, concat_axis=0)
    tab_m = served.reshape(owner_count * capacity, PLEN, 2 * HW)
    tab_o = swap(tab_m)
    mine = pick(target.reshape(N_Y, 2, -1), c, 1).reshape(-1)
    sc_attend = jnp.concatenate([mine, jnp.stack(yord)]).astype(i32)

    w_mine = [query_weight, outer_gate, inner_gate, conv_input]
    weights = w_mine + [swap(w) for w in w_mine]
    taps_part = swap(conv_taps)
    gate = route_gate_projection.T

    q, *convs, logits = project(sc_project, pieces, weights, gate, conv_taps, taps_part)
    conv_all = [convs[3], shift(convs[1], 1), shift(convs[2], -1), shift(convs[0], 2)]
    half = finish(0, sc_quarter, [conv_out] + ring, [conv_out_other] + ring_other, conv_all, logits)
    mems = attend(sc_attend, q, tab_m, tab_o)
    mem_all = [mems[3], shift(mems[1], 1), shift(mems[2], -1), shift(mems[0], 2)]
    return finish(
        1, sc_quarter, [memory_out] + ring, [memory_out_other] + ring_other, mem_all, logits, half
    )


def solution(mesh):
    return jax.shard_map(
        local,
        mesh=mesh,
        in_specs=(
            P("st", "tp"),
            P("st", None, None),
            P("st", None),
            P("st", None),
            P(None, "tp"),
            P(None, "tp"),
            P(None, "tp"),
            P(None, "tp"),
            P(None, "tp"),
            P(None, "tp"),
            P(None, "tp"),
            P(),
            P("tp", None),
            P("tp", None),
        ),
        out_specs=P(("st", "tp"), None),
        check_vma=False,
    )
```

```python
import jax
import jax.numpy as jnp
from jax import lax
from jax.experimental import pallas as pl
from jax.experimental.pallas import tpu as pltpu
from jax.sharding import PartitionSpec as P

HEAD_SIZE = 128
SEQ_LEN = 256
BLOCK = 128
NPB = 2
PLEN = 64
N_Y = 4
N_X = 4
N_Z = 4
BF = jnp.bfloat16
F32 = jnp.float32
SERVE_VMEM, PROJECT_VMEM, ATTEND_VMEM, FINISH_VMEM, SMALL_VMEM, PREP_VMEM = 58, 62, 8, 14, 6, 62


SHIFT = {
    s: [(2 * y + c, 2 * ((y + s) % N_Y) + c) for y in range(N_Y) for c in range(2)]
    for s in (1, -1, 2)
}
SWAP = [(2 * y + c, 2 * y + 1 - c) for y in range(N_Y) for c in range(2)]


def plane_shift(s):
    pairs = []
    for z in range(N_Z):
        for x in range(N_X):
            for y in range(N_Y):
                for c in range(2):
                    z2, x2 = (z, (x + s) % N_X) if c == 0 else ((z + s) % N_Z, x)
                    pairs.append(((z * N_X + x) * 8 + 2 * y + c, (z2 * N_X + x2) * 8 + 2 * y + c))
    return pairs


def shift(a, s):
    return lax.ppermute(a, "tp", SHIFT[s])


def swap(a):
    return lax.ppermute(a, "tp", SWAP)


def plane(a, s):
    return lax.ppermute(a, ("st", "tp"), plane_shift(s))


def pick(a, index, axis=0):
    return lax.dynamic_index_in_dim(a, index, axis, keepdims=False)


def dot(a, b):
    return jnp.dot(a, b, preferred_element_type=F32)


def call(body, sc, ins, in_specs, outs, out_specs, scratch=(), grid=(1,), flops=0, bytes_=0, vmem=62):
    return pl.pallas_call(
        body,
        grid_spec=pltpu.PrefetchScalarGridSpec(
            num_scalar_prefetch=1,
            grid=grid,
            in_specs=in_specs,
            out_specs=out_specs,
            scratch_shapes=list(scratch),
        ),
        out_shape=[jax.ShapeDtypeStruct(shape, dtype) for shape, dtype in outs],
        compiler_params=pltpu.CompilerParams(vmem_limit_bytes=vmem * 2**20),
        cost_estimate=pl.CostEstimate(flops=flops, bytes_accessed=bytes_, transcendentals=0),
    )(sc, *ins)


def whole(a):
    return pl.BlockSpec(a.shape, lambda *_, n=a.ndim: (0,) * n)


def fixed(*shape):
    return pl.BlockSpec(shape, lambda *_, n=len(shape): (0,) * n)


HBM = pl.BlockSpec(memory_space=pl.ANY)


def start(copies):
    for c in copies:
        c.start()


def wait(copies):
    for c in copies:
        c.wait()


def prep_kernel(sc, tokens, conv_out, memory_out, slab, other, part, quarter_s, sems):
    core, quarter = sc[2], sc[0]
    n = N_Y * SEQ_LEN
    rows = pl.ds(pl.multiple_of(quarter * 32, 32), 32)
    pairs = [
        (conv_out.at[rows], quarter_s.at[pl.ds(0, 32)]),
        (memory_out.at[rows], quarter_s.at[pl.ds(32, 32)]),
    ]
    for j in range(N_Y):
        own = pl.multiple_of((2 * j + core) * SEQ_LEN, SEQ_LEN)
        away = pl.multiple_of((2 * j + 1 - core) * SEQ_LEN, SEQ_LEN)
        dst = pl.ds(j * SEQ_LEN, SEQ_LEN)
        pairs.append((tokens.at[pl.ds(own, SEQ_LEN)], slab.at[dst]))
        pairs.append((tokens.at[pl.ds(away, SEQ_LEN)], other.at[dst]))
    copies = [pltpu.make_async_copy(x, y, sems.at[k]) for k, (x, y) in enumerate(pairs)]
    start(copies)
    wait(copies[:2])
    for cb in range(8):
        piece = quarter_s[:, cb * 256 : (cb + 1) * 256]
        slab[n + cb * 64 : n + (cb + 1) * 64] = piece
        part[cb * 64 : (cb + 1) * 64] = piece
    wait(copies[2:])


def prep(sc, tokens, conv_out, memory_out):
    n, k = N_Y * SEQ_LEN, tokens.shape[1]
    return call(
        prep_kernel, sc, (tokens, conv_out, memory_out), [HBM] * 3,
        [((n + 512, k), BF), ((n, k), BF), ((512, k), BF)],
        [fixed(n + 512, k), fixed(n, k), fixed(512, k)],
        scratch=[pltpu.VMEM((64, 2048), BF), pltpu.SemaphoreType.DMA((10,))],
        bytes_=3 * 2**20, flops=10**8, vmem=PREP_VMEM,
    )


def pack_kernel(sc, a, b, c, out):
    for d, (ref, first) in enumerate(((a, ref_rows(a)), (b, ref_rows(b)), (c, 0))):
        for cb in range(8):
            out[d * 64 : (d + 1) * 64, cb * 256 : (cb + 1) * 256] = ref[
                first + cb * 64 : first + (cb + 1) * 64
            ]


def ref_rows(ref):
    return ref.shape[0] - 512


def pack(sc, parts):
    tail = lambda a: pl.BlockSpec((512, a.shape[1]), lambda i, s, n=a.shape[0] // 512: (n - 1, 0))
    return call(
        pack_kernel, sc, parts, [tail(p) for p in parts],
        [((192, 2048), BF)], [fixed(192, 2048)], bytes_=2**20, flops=10**8, vmem=SMALL_VMEM,
    )[0]


def serve_kernel(sc, rows, kw, vw, out, table, w, sems):
    j = pl.program_id(0)
    H = kw.shape[1]

    @pl.when(j == 0)
    def _():
        w[:, :H] = kw[...]
        w[:, H:] = vw[...]

    per = rows.shape[0] // PLEN
    kv = dot(rows[...], w[...]).astype(BF)
    table[pl.ds(j * per, per)] = kv.reshape(per, PLEN, 2 * H)

    @pl.when(j == pl.num_programs(0) - 1)
    def _():
        n_own, cap = out.shape[0], out.shape[1]
        copies = [
            pltpu.make_async_copy(table.at[sc[o, k]], out.at[o, k], sems.at[o * cap + k])
            for o in range(n_own)
            for k in range(cap)
        ]
        for c in copies:
            c.start()
        for c in copies:
            c.wait()


def serve(wanted, store, kw, vw):
    n_own, cap = wanted.shape
    flat = store.reshape(-1, store.shape[-1])
    rows, d = flat.shape
    H = kw.shape[1]
    block = 512
    return call(
        serve_kernel, wanted, (flat, kw, vw),
        [pl.BlockSpec((block, d), lambda j, s: (j, 0)), whole(kw), whole(vw)],
        [((n_own, cap, PLEN, 2 * H), BF)], [HBM],
        scratch=[
            pltpu.VMEM((store.shape[0], PLEN, 2 * H), BF),
            pltpu.VMEM((d, 2 * H), BF),
            pltpu.SemaphoreType.DMA((n_own * cap,)),
        ],
        grid=(rows // block,), flops=2 * rows * d * 2 * H, bytes_=11 * 2**20, vmem=SERVE_VMEM,
    )[0]


def project_kernel(sc, *refs):
    pieces, weights = refs[:8], refs[8:16]
    gate, tm, to = refs[16:19]
    q_out, conv_outs, logit_ref = refs[19], refs[20:24], refs[24]
    lhs, w, acc, q_s, conv_s, lsem, wsem, osem = refs[25:]
    H = HEAD_SIZE
    n_rows = lhs.shape[0]
    lcopy = [
        pltpu.make_async_copy(
            p.at[pl.ds(0, n_rows)],
            lhs.at[:, pl.ds(pl.multiple_of(sc[k] * 256, 256), 256)],
            lsem.at[k],
        )
        for k, p in enumerate(pieces)
    ]
    wcopy = [
        pltpu.make_async_copy(p, w.at[n // 2, :, pl.ds(n % 2 * H, H)], wsem.at[n // 2])
        for n, p in enumerate(weights)
    ]
    start(lcopy)
    start(wcopy)
    wait(lcopy)

    def product(n, carry):
        pltpu.make_async_copy(w.at[n], w.at[n], wsem.at[n]).wait()
        acc[n] = dot(lhs[...], w[n])
        return carry

    lax.fori_loop(0, 4, product, 0)
    ids = lax.broadcasted_iota(jnp.int32, (SEQ_LEN, H), 0)
    taps = [t[...].astype(F32) for t in (tm, to)]

    def convolve(j, carry):
        rows = pl.ds(pl.multiple_of(sc[8 + j] * SEQ_LEN, SEQ_LEN), SEQ_LEN)
        for side, t in enumerate(taps):
            prod = acc[2 * side + 1, rows, :H] * acc[2 * side + 1, rows, H:]
            back1 = jnp.where(ids >= 1, pltpu.roll(prod, 1, 0), 0.0)
            back2 = jnp.where(ids >= 2, pltpu.roll(prod, 2, 0), 0.0)
            filtered = t[0:1] * back2 + t[1:2] * back1 + t[2:3] * prod
            outer = acc[2 * side, rows, H:]
            conv_s[j, :, side * H : (side + 1) * H] = (outer * filtered).astype(BF)
        return carry

    lax.fori_loop(0, 4, convolve, 0)
    ocopy = [pltpu.make_async_copy(conv_s.at[j], conv_outs[j], osem.at[j]) for j in range(4)]
    start(ocopy)
    q_s[:, :H] = acc[0, :, :H].astype(BF)
    q_s[:, H:] = acc[2, :, :H].astype(BF)
    qcopy = [pltpu.make_async_copy(q_s, q_out, osem.at[4])]
    start(qcopy)
    own = pl.ds(pl.multiple_of(sc[11] * SEQ_LEN, SEQ_LEN), SEQ_LEN)
    logit_ref[...] = lax.dot_general(
        lhs[own, :], gate[...], (((1,), (1,)), ((), ())), preferred_element_type=F32
    )
    wait(ocopy)
    wait(qcopy)


def project(sc, pieces, weights, gate, tm, to):
    rows = N_Y * SEQ_LEN
    d = gate.shape[1]
    return call(
        project_kernel, sc, (*pieces, *weights, gate, tm, to),
        [HBM] * 16 + [whole(a) for a in (gate, tm, to)],
        [((rows, 256), BF)] + [((SEQ_LEN, 256), BF)] * 4 + [((SEQ_LEN, 2), F32)],
        [HBM] * 5 + [fixed(SEQ_LEN, 2)],
        scratch=[
            pltpu.VMEM((rows, d), BF),
            pltpu.VMEM((4, d, 256), BF),
            pltpu.VMEM((4, rows, 256), F32),
            pltpu.VMEM((rows, 256), BF),
            pltpu.VMEM((4, SEQ_LEN, 256), BF),
            pltpu.SemaphoreType.DMA((8,)),
            pltpu.SemaphoreType.DMA((4,)),
            pltpu.SemaphoreType.DMA((5,)),
        ],
        flops=2 * rows * d * 1024, bytes_=10 * 2**20, vmem=PROJECT_VMEM,
    )


def attend_kernel(sc, q_in, tab_m, tab_o, *refs):
    outs = refs[:4]
    q, kv, s_ref, p_ref, sems, qsem = refs[4:]
    H = HEAD_SIZE
    qcopy = pltpu.make_async_copy(q_in, q, qsem)
    qcopy.start()
    work, copies = [], []
    for j in range(4):
        for half in range(2):
            b = sc[16 + j] * 2 + half
            rows = pl.ds(pl.multiple_of(b * BLOCK, BLOCK), BLOCK)
            for h, tab in enumerate((tab_m, tab_o)):
                i = len(work)
                for n in range(NPB):
                    copies.append(
                        pltpu.make_async_copy(
                            tab.at[sc[NPB * b + n]],
                            kv.at[i, pl.ds(n * PLEN, PLEN)],
                            sems.at[NPB * i + n],
                        )
                    )
                work.append((j, half, h, rows))
    start(copies)
    qcopy.wait()
    wait(copies)
    n = len(work)
    for i, (j, half, h, rows) in enumerate(work):
        s_ref[i * BLOCK : (i + 1) * BLOCK] = lax.dot_general(
            q[rows, h * H : (h + 1) * H], kv[i, :, :H], (((1,), (1,)), ((), ())),
            preferred_element_type=F32,
        )
    for i in range(0, n, 4):
        part = slice(i * BLOCK, (i + 4) * BLOCK)
        s = s_ref[part] * (H**-0.5)
        e = jnp.exp(s - jnp.max(s, axis=-1, keepdims=True))
        p_ref[part] = (e / jnp.sum(e, axis=-1, keepdims=True)).astype(BF)
    for i, (j, half, h, rows) in enumerate(work):
        o = dot(p_ref[i * BLOCK : (i + 1) * BLOCK], kv[i, :, H:])
        outs[j][half * BLOCK : (half + 1) * BLOCK, h * H : (h + 1) * H] = o.astype(BF)


def attend(sc, q, tab_m, tab_o):
    n = 16
    return call(
        attend_kernel, sc, (q, tab_m, tab_o), [HBM] * 3,
        [((SEQ_LEN, 256), BF)] * 4, [fixed(SEQ_LEN, 256)] * 4,
        scratch=[
            pltpu.VMEM(q.shape, BF),
            pltpu.VMEM((n, NPB * PLEN, 256), BF),
            pltpu.VMEM((n * BLOCK, BLOCK), F32),
            pltpu.VMEM((n * BLOCK, BLOCK), BF),
            pltpu.SemaphoreType.DMA((n * NPB,)),
            pltpu.SemaphoreType.DMA,
        ],
        flops=10**9, bytes_=5 * 2**20, vmem=ATTEND_VMEM,
    )


VM = pl.BlockSpec(memory_space=pltpu.VMEM)
SM = pl.BlockSpec(memory_space=pltpu.SMEM)


def plain_call(body, ins, in_specs, outs, out_specs, scratch, vmem):
    return pl.pallas_call(
        body,
        in_specs=in_specs,
        out_specs=out_specs,
        out_shape=[jax.ShapeDtypeStruct(shape, dtype) for shape, dtype in outs],
        scratch_shapes=scratch,
        compiler_params=pltpu.CompilerParams(vmem_limit_bytes=vmem * 2**20),
        cost_estimate=pl.CostEstimate(
            flops=SEQ_LEN * 2048 * 2048, bytes_accessed=7 * 2**20, transcendentals=0
        ),
    )(*ins)


def branch_product(parts, logits, branch, w, write):
    mix = jax.nn.sigmoid(logits[:, branch : branch + 1])
    x = jnp.concatenate([p[...] for p in parts], axis=1)
    step = 512

    def product(i, carry):
        cols = pl.ds(pl.multiple_of(i * step, step), step)
        write(i, cols, mix * dot(x, w[:, cols]))
        return carry

    lax.fori_loop(0, w.shape[1] // step, product, 0)


def finish0_kernel(sc, *refs):
    owns, rings = refs[0:4], (refs[4:8], refs[8:12])
    parts, logits = refs[12:16], refs[16]
    acc, w1, w0, sems = refs[17:]
    groups = []
    for branch, w in enumerate((w0, w1)):
        pairs = []
        for side in range(2):
            base = side * 128
            pairs.append((owns[2 * branch + side], w.at[pl.ds(base, 128)]))
            for src, back in zip(rings[side], (0, 3, 1, 2)):
                quarter = lax.rem(sc[side] + back, 4)
                row = pl.multiple_of(base + quarter * 32, 32)
                for d in range(3):
                    pairs.append(
                        (
                            src.at[pl.ds(d * 64 + branch * 32, 32)],
                            w.at[pl.ds((1 + d) * 256 + row, 32)],
                        )
                    )
        groups.append(
            [
                pltpu.make_async_copy(a, b, sems.at[branch * 26 + n])
                for n, (a, b) in enumerate(pairs)
            ]
        )
    start(groups[0])
    start(groups[1])
    wait(groups[0])

    def write(i, cols, a):
        acc[:, cols] = a

    branch_product(parts, logits, 0, w0, write)
    wait(groups[1])


def finish0(sc, owns, ring, ring_other, parts, logits):
    width = owns[0].shape[1]
    return plain_call(
        finish0_kernel, (sc, *owns, *ring, *ring_other, *parts, logits),
        [SM] + [HBM] * 12 + [VM] * 5,
        [((SEQ_LEN, width), F32), ((1024, width), BF)], [VM, VM],
        [pltpu.VMEM((1024, width), BF), pltpu.SemaphoreType.DMA((52,))], FINISH_VMEM,
    )


def finish1_kernel(*refs):
    parts, logits, acc, w1 = refs[0:4], refs[4], refs[5], refs[6]
    out, rows, sems = refs[7:]

    def chunk(i):
        cols = pl.ds(pl.multiple_of(i * 512, 512), 512)
        return pltpu.make_async_copy(rows.at[:, cols], out.at[:, cols], sems.at[i])

    def write(i, cols, a):
        rows[:, cols] = (acc[:, cols] + a).astype(BF)
        chunk(i).start()

    branch_product(parts, logits, 1, w1, write)
    for i in range(rows.shape[1] // 512):
        chunk(i).wait()


def finish1(parts, logits, acc, w1):
    width = w1.shape[1]
    return plain_call(
        finish1_kernel, (*parts, logits, acc, w1), [VM] * 7,
        [((SEQ_LEN, width), BF)], [HBM],
        [pltpu.VMEM((SEQ_LEN, width), BF), pltpu.SemaphoreType.DMA((width // 512,))], FINISH_VMEM,
    )[0]


def local(
    tokens,
    store,
    passage_holder_index,
    passage_slot,
    query_weight,
    key_matrix,
    value_weight,
    outer_gate,
    inner_gate,
    conv_input,
    conv_taps,
    route_gate_projection,
    conv_out,
    memory_out,
):
    me = lax.axis_index("tp")
    st = lax.axis_index("st")
    y, c = me // 2, me % 2
    z, x = st // N_X, st % N_X
    HW = query_weight.shape[1]
    i32 = jnp.int32

    quarter = jnp.where(c == 0, x, z)
    quarter_other = jnp.where(c == 0, z, x)
    sc_quarter = jnp.stack([quarter, quarter_other, c]).astype(i32)
    slab, other, part = prep(sc_quarter, tokens, conv_out, memory_out)

    a0, b0 = shift(slab, 1), shift(slab, -1)
    h1 = swap(other)
    far_part = shift(part, 2)
    a1, b1 = shift(h1, 1), shift(h1, -1)
    c0, c1 = shift(a0[: N_Y * SEQ_LEN], 1), shift(b1, -1)
    pieces = (slab, h1, a0, b0, a1, b1, c0, c1)

    e = pack(sc_quarter, (a0, b0, far_part))
    ring = [e, plane(e, 1), plane(e, -1), plane(e, 2)]
    ring_other = [swap(a) for a in ring]
    conv_out_other, memory_out_other = swap(conv_out), swap(memory_out)

    owners = passage_holder_index.reshape(-1)
    local_slots = passage_slot.reshape(-1)
    owner_count = lax.axis_size("st")
    request_count = owners.shape[0]
    capacity = max(2, 2 * request_count // owner_count)
    one_hot = (owners[:, None] == jnp.arange(owner_count, dtype=i32)[None, :]).astype(i32)
    before = jnp.cumsum(one_hot, axis=0) - one_hot
    position = jnp.sum(before * one_hot, axis=1)
    target = owners * capacity + position
    matches = (target[:, None] == jnp.arange(owner_count * capacity, dtype=i32)[None, :]).astype(i32)
    outgoing = jnp.sum(matches * local_slots[:, None], axis=0).reshape(owner_count, capacity)
    wanted = lax.all_to_all(outgoing, "st", split_axis=0, concat_axis=0)

    def slice_of(dy, flip):
        return 2 * ((y + dy) % N_Y) + (1 - c if flip else c)

    flips = ((0, False), (0, True), (-1, False), (1, False), (-1, True), (1, True), (2, False), (2, True))
    yord = [(y + d) % N_Y for d in (2, 1, -1, 0)]
    sc_project = jnp.stack([slice_of(*f) for f in flips] + yord).astype(i32)

    chosen = serve(wanted, store, key_matrix, value_weight)
    served = lax.all_to_all(chosen, "st", split_axis=0, concat_axis=0)
    tab_m = served.reshape(owner_count * capacity, PLEN, 2 * HW)
    tab_o = swap(tab_m)
    mine = pick(target.reshape(N_Y, 2, -1), c, 1).reshape(-1)
    sc_attend = jnp.concatenate([mine, jnp.stack(yord)]).astype(i32)

    w_mine = [query_weight, outer_gate, inner_gate, conv_input]
    weights = w_mine + [swap(w) for w in w_mine]
    taps_part = swap(conv_taps)
    gate = route_gate_projection.T

    q, *convs, logits = project(sc_project, pieces, weights, gate, conv_taps, taps_part)
    conv_all = [convs[3], shift(convs[1], 1), shift(convs[2], -1), shift(convs[0], 2)]
    owns = (conv_out, conv_out_other, memory_out, memory_out_other)
    acc, w1 = finish0(sc_quarter, owns, ring, ring_other, conv_all, logits)
    mems = attend(sc_attend, q, tab_m, tab_o)
    mem_all = [mems[3], shift(mems[1], 1), shift(mems[2], -1), shift(mems[0], 2)]
    return finish1(mem_all, logits, acc, w1)


def solution(mesh):
    return jax.shard_map(
        local,
        mesh=mesh,
        in_specs=(
            P("st", "tp"),
            P("st", None, None),
            P("st", None),
            P("st", None),
            P(None, "tp"),
            P(None, "tp"),
            P(None, "tp"),
            P(None, "tp"),
            P(None, "tp"),
            P(None, "tp"),
            P(None, "tp"),
            P(),
            P("tp", None),
            P("tp", None),
        ),
        out_specs=P(("st", "tp"), None),
        check_vma=False,
    )
```

```python
import jax
import jax.numpy as jnp
from jax import lax
from jax.experimental import pallas as pl
from jax.experimental.pallas import tpu as pltpu
from jax.sharding import PartitionSpec as P

HEAD_SIZE = 128
SEQ_LEN = 256
BLOCK = 128
NPB = 2
PLEN = 64
N_Y = 4
N_X = 4
N_Z = 4
BF = jnp.bfloat16
F32 = jnp.float32
SERVE_VMEM, PROJECT_VMEM, ATTEND_VMEM, FINISH_VMEM, SMALL_VMEM, PREP_VMEM = 62, 57, 8, 14, 6, 62


SHIFT = {
    s: [(2 * y + c, 2 * ((y + s) % N_Y) + c) for y in range(N_Y) for c in range(2)]
    for s in (1, -1, 2)
}
SWAP = [(2 * y + c, 2 * y + 1 - c) for y in range(N_Y) for c in range(2)]


def plane_shift(s):
    pairs = []
    for z in range(N_Z):
        for x in range(N_X):
            for y in range(N_Y):
                for c in range(2):
                    z2, x2 = (z, (x + s) % N_X) if c == 0 else ((z + s) % N_Z, x)
                    pairs.append(((z * N_X + x) * 8 + 2 * y + c, (z2 * N_X + x2) * 8 + 2 * y + c))
    return pairs


def shift(a, s):
    return lax.ppermute(a, "tp", SHIFT[s])


def swap(a):
    return lax.ppermute(a, "tp", SWAP)


def plane(a, s):
    return lax.ppermute(a, ("st", "tp"), plane_shift(s))


def dot(a, b):
    return jnp.dot(a, b, preferred_element_type=F32)


def call(body, sc, ins, in_specs, outs, out_specs, scratch=(), grid=(1,), flops=0, bytes_=0, vmem=62):
    return pl.pallas_call(
        body,
        grid_spec=pltpu.PrefetchScalarGridSpec(
            num_scalar_prefetch=1,
            grid=grid,
            in_specs=in_specs,
            out_specs=out_specs,
            scratch_shapes=list(scratch),
        ),
        out_shape=[jax.ShapeDtypeStruct(shape, dtype) for shape, dtype in outs],
        compiler_params=pltpu.CompilerParams(vmem_limit_bytes=vmem * 2**20),
        cost_estimate=pl.CostEstimate(flops=flops, bytes_accessed=bytes_, transcendentals=0),
    )(sc, *ins)


def whole(a):
    return pl.BlockSpec(a.shape, lambda *_, n=a.ndim: (0,) * n)


def fixed(*shape):
    return pl.BlockSpec(shape, lambda *_, n=len(shape): (0,) * n)


HBM = pl.BlockSpec(memory_space=pl.ANY)


def start(copies):
    for c in copies:
        c.start()


def wait(copies):
    for c in copies:
        c.wait()


def place():
    me, st = lax.axis_index("tp"), lax.axis_index("st")
    y, c, z, x = lax.div(me, 2), lax.rem(me, 2), lax.div(st, N_X), lax.rem(st, N_X)
    first, second = lax.select(c == 0, x, z), lax.select(c == 0, z, x)
    return y, c, first, second


def prep_kernel(sc, tokens, conv_out, memory_out, mine, other, part, sems):
    _, core, quarter, _ = place()
    rows = pl.ds(pl.multiple_of(quarter * 32, 32), 32)
    pairs = [
        (conv_out.at[rows], part.at[pl.ds(0, 32)]),
        (memory_out.at[rows], part.at[pl.ds(32, 32)]),
    ]
    for j in range(N_Y):
        own = pl.multiple_of((2 * j + core) * SEQ_LEN, SEQ_LEN)
        away = pl.multiple_of((2 * j + 1 - core) * SEQ_LEN, SEQ_LEN)
        dst = pl.ds(j * SEQ_LEN, SEQ_LEN)
        pairs.append((tokens.at[pl.ds(own, SEQ_LEN)], mine.at[dst]))
        pairs.append((tokens.at[pl.ds(away, SEQ_LEN)], other.at[dst]))
    copies = [pltpu.make_async_copy(x, y, sems.at[k]) for k, (x, y) in enumerate(pairs)]
    start(copies)
    wait(copies)


def prep(sc, tokens, conv_out, memory_out):
    n, k = N_Y * SEQ_LEN, tokens.shape[1]
    d = conv_out.shape[1]
    return call(
        prep_kernel, sc, (tokens, conv_out, memory_out), [HBM] * 3,
        [((n, k), BF), ((n, k), BF), ((64, d), BF)],
        [fixed(n, k), fixed(n, k), fixed(64, d)],
        scratch=[pltpu.SemaphoreType.DMA((10,))], bytes_=3 * 2**20, flops=10**8, vmem=PREP_VMEM,
    )


def pack_kernel(sc, a, b, c, out):
    n = a.shape[0]
    for d, ref in enumerate((a, b, c)):
        out[d * n : (d + 1) * n] = ref[...]


def pack(sc, parts):
    n, d = parts[0].shape
    return call(
        pack_kernel, sc, parts, [whole(p) for p in parts],
        [((3 * n, d), BF)], [fixed(3 * n, d)], bytes_=2**20, flops=10**8, vmem=SMALL_VMEM,
    )[0]


def serve_kernel(sc, rows, kw, vw, out, table, w):
    j = pl.program_id(0)
    H = kw.shape[1]

    @pl.when(j == 0)
    def _():
        w[:, :H] = kw[...]
        w[:, H:] = vw[...]

    per = rows.shape[0] // PLEN
    kv = dot(rows[...], w[...]).astype(BF)
    table[pl.ds(j * per, per)] = kv.reshape(per, PLEN, 2 * H)

    @pl.when(j == pl.num_programs(0) - 1)
    def _():
        for o in range(out.shape[0]):
            for k in range(out.shape[1]):
                out[o, k] = table[sc[o, k]]


def serve(wanted, store, kw, vw):
    n_own, cap = wanted.shape
    flat = store.reshape(-1, store.shape[-1])
    rows, d = flat.shape
    H = kw.shape[1]
    block = 1024
    return call(
        serve_kernel, wanted, (flat, kw, vw),
        [pl.BlockSpec((block, d), lambda j, s: (j, 0)), whole(kw), whole(vw)],
        [((n_own, cap, PLEN, 2 * H), BF)], [fixed(n_own, cap, PLEN, 2 * H)],
        scratch=[
            pltpu.VMEM((store.shape[0], PLEN, 2 * H), BF),
            pltpu.VMEM((d, 2 * H), BF),
        ],
        grid=(rows // block,), flops=2 * rows * d * 2 * H, bytes_=11 * 2**20, vmem=SERVE_VMEM,
    )[0]


def project_kernel(_, *refs):
    y, c, *_ = place()
    sc = [
        2 * lax.rem(y + d, N_Y) + (1 - c if flip else c)
        for d, flip in ((0, 0), (0, 1), (3, 0), (1, 0), (3, 1), (1, 1), (2, 0), (2, 1))
    ]
    pieces, weights = refs[:8], refs[8:16]
    gate, tm, to = refs[16:19]
    q_out, conv_outs, logit_ref = refs[19], refs[20:24], refs[24]
    lhs, w, acc, q_s, conv_s, lsem, wsem, osem = refs[25:]
    H = HEAD_SIZE
    n_rows = lhs.shape[1]
    lcopy = [
        pltpu.make_async_copy(
            p.at[pl.ds(0, n_rows)], lhs.at[sc[k]], lsem.at[k]
        )
        for k, p in enumerate(pieces)
    ]
    wcopy = [
        pltpu.make_async_copy(p, w.at[n // 2, n % 2], wsem.at[n // 2])
        for n, p in enumerate(weights)
    ]
    start(wcopy[:2])
    start(lcopy)
    wait(lcopy)
    start(wcopy[2:])

    def product(n, carry):
        pltpu.make_async_copy(w.at[n], w.at[n], wsem.at[n]).wait()
        x = jnp.concatenate([lhs[k] for k in range(8)], axis=1)
        acc[n] = dot(x, jnp.concatenate([w[n, 0], w[n, 1]], axis=1))
        return carry

    lax.fori_loop(0, 4, product, 0)
    ids = lax.broadcasted_iota(jnp.int32, (SEQ_LEN, H), 0)
    taps = [t[...].astype(F32) for t in (tm, to)]

    def rel(j):
        return lax.rem(y + jnp.where(j == 0, 2, jnp.where(j == 1, 1, jnp.where(j == 2, 3, 0))), N_Y)

    def convolve(j, carry):
        rows = pl.ds(pl.multiple_of(rel(j) * SEQ_LEN, SEQ_LEN), SEQ_LEN)
        for side, t in enumerate(taps):
            prod = acc[2 * side + 1, rows, :H] * acc[2 * side + 1, rows, H:]
            back1 = jnp.where(ids >= 1, pltpu.roll(prod, 1, 0), 0.0)
            back2 = jnp.where(ids >= 2, pltpu.roll(prod, 2, 0), 0.0)
            filtered = t[0:1] * back2 + t[1:2] * back1 + t[2:3] * prod
            outer = acc[2 * side, rows, H:]
            conv_s[j, :, side * H : (side + 1) * H] = (outer * filtered).astype(BF)
        return carry

    lax.fori_loop(0, 4, convolve, 0)
    ocopy = [pltpu.make_async_copy(conv_s.at[j], conv_outs[j], osem.at[j]) for j in range(4)]
    start(ocopy)
    q_s[:, :H] = acc[0, :, :H].astype(BF)
    q_s[:, H:] = acc[2, :, :H].astype(BF)
    qcopy = [pltpu.make_async_copy(q_s, q_out, osem.at[4])]
    start(qcopy)
    own = pl.ds(pl.multiple_of(y * SEQ_LEN, SEQ_LEN), SEQ_LEN)
    logit_ref[...] = lax.dot_general(
        jnp.concatenate([lhs[k, own, :] for k in range(8)], axis=1), gate[...], (((1,), (1,)), ((), ())), preferred_element_type=F32
    )
    wait(ocopy)
    wait(qcopy)


def project(sc, pieces, weights, gate, tm, to):
    rows = N_Y * SEQ_LEN
    d = gate.shape[1]
    return call(
        project_kernel, sc, (*pieces, *weights, gate, tm, to),
        [HBM] * 16 + [whole(a) for a in (gate, tm, to)],
        [((rows, 256), BF)] + [((SEQ_LEN, 256), BF)] * 4 + [((SEQ_LEN, 2), F32)],
        [HBM] * 5 + [fixed(SEQ_LEN, 2)],
        scratch=[
            pltpu.VMEM((8, rows, 256), BF),
            pltpu.VMEM((4, 2, d, 128), BF),
            pltpu.VMEM((4, rows, 256), F32),
            pltpu.VMEM((rows, 256), BF),
            pltpu.VMEM((4, SEQ_LEN, 256), BF),
            pltpu.SemaphoreType.DMA((8,)),
            pltpu.SemaphoreType.DMA((4,)),
            pltpu.SemaphoreType.DMA((5,)),
        ],
        flops=2 * rows * d * 1024, bytes_=10 * 2**20, vmem=PROJECT_VMEM,
    )


def attend_kernel(sc, q_in, tab_m, tab_o, *refs):
    outs = refs[:4]
    q, kv, s_ref, p_ref, sems, qsem = refs[4:]
    y, c, *_ = place()
    H = HEAD_SIZE
    qcopy = pltpu.make_async_copy(q_in, q, qsem)
    qcopy.start()
    work, copies = [], []
    for j in range(4):
        for half in range(2):
            b = lax.rem(y + (2, 1, 3, 0)[j], N_Y) * 2 + half
            read = NPB * (lax.div(b, 2) * 4 + c * 2 + half)
            rows = pl.ds(pl.multiple_of(b * BLOCK, BLOCK), BLOCK)
            for h, tab in enumerate((tab_m, tab_o)):
                i = len(work)
                for n in range(NPB):
                    copies.append(
                        pltpu.make_async_copy(
                            tab.at[sc[read + n]],
                            kv.at[i, pl.ds(n * PLEN, PLEN)],
                            sems.at[NPB * i + n],
                        )
                    )
                work.append((j, half, h, rows))
    start(copies)
    qcopy.wait()
    wait(copies)
    n = len(work)
    for i, (j, half, h, rows) in enumerate(work):
        s_ref[i * BLOCK : (i + 1) * BLOCK] = lax.dot_general(
            q[rows, h * H : (h + 1) * H], kv[i, :, :H], (((1,), (1,)), ((), ())),
            preferred_element_type=F32,
        )
    for i in range(0, n, 4):
        part = slice(i * BLOCK, (i + 4) * BLOCK)
        s = s_ref[part] * (H**-0.5)
        e = jnp.exp(s - jnp.max(s, axis=-1, keepdims=True))
        p_ref[part] = (e / jnp.sum(e, axis=-1, keepdims=True)).astype(BF)
    for i, (j, half, h, rows) in enumerate(work):
        o = dot(p_ref[i * BLOCK : (i + 1) * BLOCK], kv[i, :, H:])
        outs[j][half * BLOCK : (half + 1) * BLOCK, h * H : (h + 1) * H] = o.astype(BF)


def attend(sc, q, tab_m, tab_o):
    n = 16
    return call(
        attend_kernel, sc, (q, tab_m, tab_o), [HBM] * 3,
        [((SEQ_LEN, 256), BF)] * 4, [fixed(SEQ_LEN, 256)] * 4,
        scratch=[
            pltpu.VMEM(q.shape, BF),
            pltpu.VMEM((n, NPB * PLEN, 256), BF),
            pltpu.VMEM((n * BLOCK, BLOCK), F32),
            pltpu.VMEM((n * BLOCK, BLOCK), BF),
            pltpu.SemaphoreType.DMA((n * NPB,)),
            pltpu.SemaphoreType.DMA,
        ],
        flops=10**9, bytes_=5 * 2**20, vmem=ATTEND_VMEM,
    )


VM = pl.BlockSpec(memory_space=pltpu.VMEM)
SM = pl.BlockSpec(memory_space=pltpu.SMEM)


def plain_call(body, ins, in_specs, outs, out_specs, scratch, vmem):
    return pl.pallas_call(
        body,
        in_specs=in_specs,
        out_specs=out_specs,
        out_shape=[jax.ShapeDtypeStruct(shape, dtype) for shape, dtype in outs],
        scratch_shapes=scratch,
        compiler_params=pltpu.CompilerParams(vmem_limit_bytes=vmem * 2**20),
        cost_estimate=pl.CostEstimate(
            flops=SEQ_LEN * 2048 * 2048, bytes_accessed=7 * 2**20, transcendentals=0
        ),
    )(*ins)


def branch_product(parts, logits, branch, w, write):
    mix = jax.nn.sigmoid(logits[:, branch : branch + 1])
    x = jnp.concatenate([p[...] for p in parts], axis=1)
    step = 512

    def product(i, carry):
        cols = pl.ds(pl.multiple_of(i * step, step), step)
        write(i, cols, mix * dot(x, w[:, cols]))
        return carry

    lax.fori_loop(0, w.shape[1] // step, product, 0)


def finish0_kernel(*refs):
    sc = place()[2:]
    owns, rings = refs[0:4], (refs[4:8], refs[8:12])
    parts, logits = refs[12:16], refs[16]
    acc, w1, w0, sems = refs[17:]
    groups = []
    for branch, w in enumerate((w0, w1)):
        pairs = []
        for side in range(2):
            base = side * 128
            pairs.append((owns[2 * branch + side], w.at[pl.ds(base, 128)]))
            for src, back in zip(rings[side], (0, 3, 1, 2)):
                quarter = lax.rem(sc[side] + back, 4)
                row = pl.multiple_of(base + quarter * 32, 32)
                for d in range(3):
                    pairs.append(
                        (
                            src.at[pl.ds(d * 64 + branch * 32, 32)],
                            w.at[pl.ds((1 + d) * 256 + row, 32)],
                        )
                    )
        groups.append(
            [
                pltpu.make_async_copy(a, b, sems.at[branch * 26 + n])
                for n, (a, b) in enumerate(pairs)
            ]
        )
    start(groups[0])
    start(groups[1])
    wait(groups[0])

    def write(i, cols, a):
        acc[:, cols] = a

    branch_product(parts, logits, 0, w0, write)
    wait(groups[1])


def finish0(owns, ring, ring_other, parts, logits):
    width = owns[0].shape[1]
    return plain_call(
        finish0_kernel, (*owns, *ring, *ring_other, *parts, logits),
        [HBM] * 12 + [VM] * 5,
        [((SEQ_LEN, width), F32), ((1024, width), BF)], [VM, VM],
        [pltpu.VMEM((1024, width), BF), pltpu.SemaphoreType.DMA((52,))], FINISH_VMEM,
    )


def finish1_kernel(*refs):
    parts, logits, acc, w1 = refs[0:4], refs[4], refs[5], refs[6]
    out, rows, sems = refs[7:]

    def chunk(i):
        cols = pl.ds(pl.multiple_of(i * 512, 512), 512)
        return pltpu.make_async_copy(rows.at[:, cols], out.at[:, cols], sems.at[i])

    def write(i, cols, a):
        rows[:, cols] = (acc[:, cols] + a).astype(BF)
        chunk(i).start()

    branch_product(parts, logits, 1, w1, write)
    for i in range(rows.shape[1] // 512):
        chunk(i).wait()


def finish1(parts, logits, acc, w1):
    width = w1.shape[1]
    return plain_call(
        finish1_kernel, (*parts, logits, acc, w1), [VM] * 7,
        [((SEQ_LEN, width), BF)], [HBM],
        [pltpu.VMEM((SEQ_LEN, width), BF), pltpu.SemaphoreType.DMA((width // 512,))], FINISH_VMEM,
    )[0]


def local(
    tokens,
    store,
    passage_holder_index,
    passage_slot,
    query_weight,
    key_matrix,
    value_weight,
    outer_gate,
    inner_gate,
    conv_input,
    conv_taps,
    route_gate_projection,
    conv_out,
    memory_out,
):
    HW = query_weight.shape[1]
    i32 = jnp.int32

    nothing = jnp.zeros((1,), i32)
    h0, other, part = prep(nothing, tokens, conv_out, memory_out)
    ys = [shift(part, d) for d in (1, -1, 2)]

    a0, b0 = shift(h0, 1), shift(h0, -1)
    h1 = swap(other)
    a1, b1 = shift(h1, 1), shift(h1, -1)
    c0, c1 = shift(a0, 1), shift(b1, -1)
    pieces = (h0, h1, a0, b0, a1, b1, c0, c1)

    e = pack(nothing, ys)
    ring = [e, plane(e, 1), plane(e, -1), plane(e, 2)]
    ring_other = [swap(a) for a in ring]
    conv_out_other, memory_out_other = swap(conv_out), swap(memory_out)

    owners = passage_holder_index.reshape(-1)
    local_slots = passage_slot.reshape(-1)
    owner_count = lax.axis_size("st")
    request_count = owners.shape[0]
    capacity = max(2, 2 * request_count // owner_count)
    one_hot = (owners[:, None] == jnp.arange(owner_count, dtype=i32)[None, :]).astype(i32)
    before = jnp.cumsum(one_hot, axis=0) - one_hot
    position = jnp.sum(before * one_hot, axis=1)
    target = owners * capacity + position
    matches = (target[:, None] == jnp.arange(owner_count * capacity, dtype=i32)[None, :]).astype(i32)
    outgoing = jnp.sum(matches * local_slots[:, None], axis=0).reshape(owner_count, capacity)
    wanted = lax.all_to_all(outgoing, "st", split_axis=0, concat_axis=0)

    chosen = serve(wanted, store, key_matrix, value_weight)
    served = lax.all_to_all(chosen, "st", split_axis=0, concat_axis=0)
    tab_m = served.reshape(owner_count * capacity, PLEN, 2 * HW)
    tab_o = swap(tab_m)

    w_mine = [query_weight, outer_gate, inner_gate, conv_input]
    weights = w_mine + [swap(w) for w in w_mine]
    taps_part = swap(conv_taps)
    gate = route_gate_projection.T

    q, *convs, logits = project(nothing, pieces, weights, gate, conv_taps, taps_part)
    conv_all = [convs[3], shift(convs[1], 1), shift(convs[2], -1), shift(convs[0], 2)]
    owns = (conv_out, conv_out_other, memory_out, memory_out_other)
    acc, w1 = finish0(owns, ring, ring_other, conv_all, logits)
    mems = attend(target, q, tab_m, tab_o)
    mem_all = [mems[3], shift(mems[1], 1), shift(mems[2], -1), shift(mems[0], 2)]
    return finish1(mem_all, logits, acc, w1)


def solution(mesh):
    return jax.shard_map(
        local,
        mesh=mesh,
        in_specs=(
            P("st", "tp"),
            P("st", None, None),
            P("st", None),
            P("st", None),
            P(None, "tp"),
            P(None, "tp"),
            P(None, "tp"),
            P(None, "tp"),
            P(None, "tp"),
            P(None, "tp"),
            P(None, "tp"),
            P(),
            P("tp", None),
            P("tp", None),
        ),
        out_specs=P(("st", "tp"), None),
        check_vma=False,
    )
```
